256 devices in a mesh: sp: 64 (over z, y, core), tp: 4 (over x).
Axes of the slice: x: 4, y: 4, z: 8, core: 2. Of those that a mesh axis runs over, the one named last changes fastest.
Arguments:
- query: bfloat16 [16384, 1536], P('sp', 'tp'), may hold values from -6 to 6
- forget_preact: bfloat16 [16384, 1536], P('sp', 'tp'), may hold values from -6 to 6
- value_input: bfloat16 [16384, 1536], P('sp', 'tp'), may hold values from -6 to 6
- output_gate: bfloat16 [16384, 1536], P('sp', 'tp'), may hold values from -6 to 6
- forget_minimum: float32 [1536], P('tp'), may hold values from 0.88 to 1
- extra_log_decay: float32 [12, 16384], P('tp', 'sp'), may hold values from -0.7 to 0
- head_norm_gain: float32 [1536], P('tp'), may hold values from 0.1 to 1.9
- output_weight: bfloat16 [1536, 3072], P(None, 'tp'), may hold values from -0.15625 to 0.15625
- stream: bfloat16 [16384, 3072], P(('sp', 'tp')), may hold values from -6 to 6
- feedforward_gain: float32 [3072], replicated, may hold values from 0.1 to 1.9
- routes: int32 [16384, 2], P('sp'), may hold values from 0 to 63, all different within a row; in each aligned block of 64 rows (0 to 63, 64 to 127, ...) at most 4 rows name the same one
- router_weight: float32 [16384, 2], P(('sp', 'tp')), may hold values from 0.05 to 1
- expert_gate_weight: bfloat16 [64, 3072, 1024], P('sp', None, 'tp'), may hold values from -0.109375 to 0.109375
- expert_up_weight: bfloat16 [64, 3072, 1024], P('sp', None, 'tp'), may hold values from -0.109375 to 0.109375
- expert_down_weight: bfloat16 [64, 1024, 3072], P('sp', 'tp'), may hold values from -0.1875 to 0.1875
Outputs:
- result: bfloat16 [16384, 3072], P(('sp', 'tp'))
The draws below stay inside these ranges and needn't reach their ends.
Inputs may be any that keep to these rules, and one draw needn't show every extreme that they name: `routes`: each row names 2 different experts; in each aligned block of 64 rows no expert is named by more than 4 rows, a bound that some block reaches.
All inputs are finite; a program needn't handle non-finite values.
Results may differ from the reference program's by a relative error of at most 0.01.
Values may be sent and summed in bfloat16 or wider, within the bound.
A program may use at most 64 MiB of HBM per device.

```python
import math
import jax
import jax.numpy as jnp
import numpy as np
from jax import lax

D = 3072
HEADS = 12
STATE_ROW_COUNT = 128
VALUE_CHANNELS = 128
FF = 1024
SPAN = 64
TOPK = 2
TOK_DEV = 256
SEQUENCE_TOKENS = 16384
KEY_WIDTH = 1536
VALUE_WIDTH = 1536
EXPERTS = 64
QROWS = 64
CAPQ = 4
N_TP = 4


def draw_forget_preact(key, part):
    base_key, shift_key = jax.random.split(key)
    base_draw = jax.random.normal(base_key, (SEQUENCE_TOKENS, KEY_WIDTH), jnp.float32)
    shift_draw = jax.random.uniform(shift_key, (SEQUENCE_TOKENS // TOK_DEV, 1), jnp.float32, -1.0, 1.0)
    shifted = base_draw + jnp.repeat(shift_draw, TOK_DEV, axis=0)
    return jnp.clip(shifted, -6.0, 6.0).astype(jnp.bfloat16)


def draw_forget_minimum(key, part):
    pick_key, slow_key, fast_key = jax.random.split(key, 3)
    slow_share = 0.5
    slow_head = jax.random.uniform(pick_key, (HEADS, 1), jnp.float32) < slow_share
    slow_rate = jnp.exp(jax.random.uniform(slow_key, (HEADS, STATE_ROW_COUNT), jnp.float32, jnp.log(0.2), jnp.log(2.0))) / SEQUENCE_TOKENS
    fast_rate = jnp.exp(jax.random.uniform(fast_key, (HEADS, STATE_ROW_COUNT), jnp.float32, jnp.log(0.04), jnp.log(0.12)))
    decay_rate = jnp.where(slow_head, slow_rate, fast_rate)
    return (1.0 - decay_rate).reshape(HEADS * STATE_ROW_COUNT).astype(jnp.float32)


def draw_extra_log_decay(key, part):
    location_seed, size_key = jax.random.split(key)
    spike_places = jax.random.randint(location_seed, (4,), 0, SEQUENCE_TOKENS)
    spike_mask = jnp.any(jnp.arange(SEQUENCE_TOKENS)[None, :] == spike_places[:, None], axis=0)
    retained_fraction = jax.random.uniform(size_key, (HEADS, 1), jnp.float32, 0.5, 0.8)
    return jnp.where(spike_mask[None, :], jnp.log(retained_fraction), 0.0).astype(jnp.float32)


def level_of(rng, dims, shards, least, largest):
    level = 1.0
    for dim, blocks in shards:
        heights = jax.random.uniform(jax.random.fold_in(jax.random.fold_in(rng, 6), dim), (blocks,), jnp.float32, least / len(shards), largest / len(shards))
        level = level * jnp.repeat(jnp.exp(heights), dims[dim] // blocks).reshape((-1,) + (1,) * (len(dims) - 1 - dim))
    return level


def assign_block(key, own, number, rows, number_of, top, reach, skew):
    ranking = jax.random.permutation(key, number_of)
    heavy_load, ordinary = portions_of(number_of, rows * top, reach, skew, True), portions_of(number_of, rows * top, reach, skew, False)
    places = jnp.arange(number_of)

    def named(tallies, rotation):
        used = int((tallies > 0).sum())
        fixed = max(1, used // 4)
        passed = fixed + (places - fixed + rotation * (used - fixed)) % max(1, number_of - fixed)
        return jnp.zeros((number_of,), jnp.int32).at[ranking[jnp.where(places < fixed, places, passed)]].set(jnp.asarray(tallies, jnp.int32))

    tallies = jnp.where(number % 4 == 0, named(heavy_load, number // 4), named(ordinary, number - number // 4 - 1))
    mixed = jax.random.permutation(jax.random.fold_in(own, 3), number_of)
    giver, taker = mixed[0:number_of // 2 * 2:2], mixed[1:number_of // 2 * 2:2]
    slack = jnp.minimum(tallies[giver] - 1, reach - tallies[taker]) // 2
    slack = jnp.where((giver == ranking[0]) | (taker == ranking[0]) | (tallies[taker] == 0), 0, jnp.maximum(slack, 0))
    passed = jax.random.randint(jax.random.fold_in(own, 4), (number_of // 2,), 0, 1 << 20) % (slack + 1)
    tallies = tallies.at[giver].add(-passed).at[taker].add(passed)
    members = jnp.searchsorted(jnp.cumsum(tallies), jnp.arange(rows * top), side="right").astype(jnp.int32)
    listing = members.reshape(top, rows).T
    listing = listing[jax.random.permutation(jax.random.fold_in(own, 1), rows)]
    rotation = jax.random.randint(jax.random.fold_in(own, 2), (rows, 1), 0, top)
    return jnp.take_along_axis(listing, (jnp.arange(top)[None, :] + rotation) % top, axis=1)


def portions_of(number_of, total, bound, lean, full):
    portions = [(1 << 20) // math.isqrt(standing ** lean) + 1 for standing in range(1, number_of + 1)]
    largest = bound if full else min(bound, max(-(-total // number_of), total * portions[0] // sum(portions)))
    least = 1 if total - largest >= number_of - 1 else 0
    holding, rest = [largest] + [least] * (number_of - 1), total - largest - least * (number_of - 1)
    while rest > 0:
        candidates = [i for i in range(1, number_of) if holding[i] < largest] or [i for i in range(1, number_of) if holding[i] < bound]
        pool, budget = sum([portions[i] for i in candidates]), rest
        for i in candidates:
            addition = min(bound - holding[i], max(1, budget * portions[i] // pool), rest)
            holding[i] = holding[i] + addition
            rest = rest - addition
    return np.array(holding)


def noise(rng, dims, scale, limit, pieces=(), kind=jnp.bfloat16):
    loudness = level_of(rng, dims, pieces, -0.22, 0.18) if pieces else 1.0
    values = jax.random.normal(rng, dims, jnp.float32) * scale * loudness
    return jnp.minimum(jnp.maximum(values, -limit), limit).astype(kind)


def setup_inputs(seed: int = 0) -> dict:
    streams_of = jax.random.split(jax.random.key(seed), 16)
    query = noise(streams_of[0], (SEQUENCE_TOKENS, KEY_WIDTH), 1.0, 6.0, ((0, 64), (1, 4)))
    forget_preact = draw_forget_preact(jax.random.fold_in(streams_of[15], 71), 0)
    value_input = noise(streams_of[2], (SEQUENCE_TOKENS, VALUE_WIDTH), 1.0, 6.0, ((0, 64), (1, 4)))
    output_gate = noise(streams_of[3], (SEQUENCE_TOKENS, VALUE_WIDTH), 1.0, 6.0, ((0, 64), (1, 4)))
    forget_minimum = draw_forget_minimum(jax.random.fold_in(streams_of[15], 71), 0)
    extra_log_decay = draw_extra_log_decay(jax.random.fold_in(streams_of[15], 71), 0)
    head_norm_gain = jnp.clip(1.0 + 0.18 * jax.random.normal(streams_of[6], (VALUE_WIDTH,), jnp.float32), 0.1, 1.9)
    output_weight = noise(streams_of[7], (VALUE_WIDTH, D), VALUE_WIDTH ** -0.5, 0.15625, ((1, 4),))
    stream = noise(streams_of[8], (SEQUENCE_TOKENS, D), 1.0, 6.0, ((0, 256),))
    feedforward_gain = jnp.clip(1.0 + 0.18 * jax.random.normal(streams_of[9], (D,), jnp.float32), 0.1, 1.9)
    routes_keys = jax.random.split(jax.random.fold_in(streams_of[10], 1), SEQUENCE_TOKENS // QROWS)
    routes_turns = jax.random.permutation(jax.random.fold_in(streams_of[10], 3), SEQUENCE_TOKENS // QROWS)
    routes = jax.vmap(lambda own, number: assign_block(jax.random.fold_in(streams_of[10], 2), own, number, QROWS, EXPERTS, TOPK, CAPQ, 2))(routes_keys, routes_turns).reshape((SEQUENCE_TOKENS, TOPK))
    router_weight = jnp.clip(0.05 + 0.95 * jax.random.uniform(streams_of[11], (SEQUENCE_TOKENS, TOPK), jnp.float32) ** level_of(streams_of[11], (SEQUENCE_TOKENS, TOPK), ((0, 256),), -0.2, 0.2), 0.05, 1.0)
    expert_gate_weight = noise(streams_of[12], (EXPERTS, D, FF), D ** -0.5, 0.109375, ((0, 64), (2, 4)))
    expert_up_weight = noise(streams_of[13], (EXPERTS, D, FF), D ** -0.5, 0.109375, ((0, 64), (2, 4)))
    expert_down_weight = noise(streams_of[14], (EXPERTS, FF, D), FF ** -0.5, 0.1875, ((0, 64), (1, 4)))
    return dict(query=query, forget_preact=forget_preact, value_input=value_input, output_gate=output_gate, forget_minimum=forget_minimum, extra_log_decay=extra_log_decay, head_norm_gain=head_norm_gain, output_weight=output_weight, stream=stream, feedforward_gain=feedforward_gain, routes=routes, router_weight=router_weight, expert_gate_weight=expert_gate_weight, expert_up_weight=expert_up_weight, expert_down_weight=expert_down_weight)


epsilon = 1e-06
top_precision = lax.Precision.HIGHEST
tile_rows = 256

def block_step(current_state, block_inputs):
    query_block, weight_blk, value_block, decay_blk = block_inputs
    running_decay = jnp.cumsum(decay_blk, axis=1)
    intermediate = jnp.einsum('yro,yow->yrw', query_block * jnp.exp(running_decay), current_state, precision=top_precision)
    causal = lax.broadcasted_iota(jnp.int32, (SPAN, SPAN), 0) >= lax.broadcasted_iota(jnp.int32, (SPAN, SPAN), 1)
    log_gap = running_decay[:, :, None, :] - running_decay[:, None, :, :]
    decay_table = jnp.exp(jnp.where(causal[None, :, :, None], log_gap, -jnp.inf))
    scores = jnp.einsum('htk,hsk,htsk->hts', query_block, weight_blk, decay_table, precision=top_precision)
    output = intermediate + jnp.einsum('hts,hsv->htv', scores, value_block, precision=top_precision)
    final_decay = running_decay[:, -1:, :]
    scaled_rows = weight_blk * jnp.exp(final_decay - running_decay)
    following_state = jnp.exp(final_decay[:, 0, :])[:, :, None] * current_state + jnp.einsum('xme,xmc->xec', scaled_rows, value_block, precision=top_precision)
    return (following_state, output)

def gate_factors(query, forget_preact, forget_minimum, extra_log_decay):
    query_activated = jax.nn.silu(query.astype(jnp.float32))
    incoming_weight = (1.0 - forget_minimum) * jax.nn.sigmoid(-forget_preact.astype(jnp.float32))
    spike_columns = jnp.repeat(jnp.transpose(extra_log_decay), STATE_ROW_COUNT, axis=1)
    decay_logarithm = jnp.log1p(-incoming_weight) + spike_columns
    return (query_activated, incoming_weight, decay_logarithm)

def head_blocks(array_in, head_total):
    rows_in = array_in.shape[0]
    return array_in.reshape(rows_in // SPAN, SPAN, head_total, -1).transpose(0, 2, 1, 3)

def head_output(mixed, head_norm_gain, output_gate):
    normalized = mixed * lax.rsqrt(lax.optimization_barrier(jnp.mean(mixed * mixed, axis=-1, keepdims=True)) + epsilon)
    flat_rows = normalized.reshape(mixed.shape[0], -1)
    return (flat_rows * head_norm_gain * jax.nn.silu(output_gate.astype(jnp.float32))).astype(jnp.bfloat16)

def rms_norm(residual, gain):
    scale_row = lax.rsqrt(lax.optimization_barrier(jnp.mean(residual * residual, axis=-1, keepdims=True)) + epsilon)
    return (residual * scale_row * gain).astype(jnp.bfloat16)

def expert_rows(row_data, gate_w, up_w, down_w):
    gate_act = jnp.dot(row_data, gate_w, preferred_element_type=jnp.float32)
    up_act = jnp.dot(row_data, up_w, preferred_element_type=jnp.float32)
    inner_act = (jax.nn.silu(gate_act) * up_act).astype(jnp.bfloat16)
    quarter = inner_act.shape[1] // N_TP
    parts = jnp.einsum('njf,jfd->njd', inner_act.reshape(-1, N_TP, quarter).astype(jnp.float32), down_w.reshape(N_TP, quarter, -1).astype(jnp.float32))
    parts = lax.optimization_barrier(parts.astype(jnp.bfloat16))
    return lax.optimization_barrier(jnp.sum(parts.astype(jnp.float32), axis=1)).astype(jnp.bfloat16)

def routed(normed, routes, route_weight, expert_gate_weight, expert_up_weight, expert_down_weight):
    pick_ids = routes.reshape(-1).astype(jnp.int32)
    flat_weight = route_weight.reshape(-1)
    expert_ids = jnp.arange(EXPERTS, dtype=jnp.int32)
    counts = lax.optimization_barrier(jnp.sum((pick_ids[:, None] == expert_ids[None, :]).astype(jnp.int32), axis=0)).astype(jnp.int32)
    starts = (jnp.cumsum(counts) - counts).astype(jnp.int32)
    sort_order = jnp.argsort(pick_ids, stable=True).astype(jnp.int32)
    padded = jnp.concatenate([sort_order, jnp.zeros((tile_rows,), jnp.int32)])
    result = jnp.zeros((normed.shape[0], normed.shape[1]), jnp.float32)

    def per_expert(expert_id, result_now):
        tile_count = ((counts[expert_id] + tile_rows - 1) // tile_rows).astype(jnp.int32)

        def per_tile(tile_id, result_tile):
            offset = (tile_id * tile_rows).astype(jnp.int32)
            row_ids = lax.dynamic_slice_in_dim(padded, (starts[expert_id] + offset).astype(jnp.int32), tile_rows)
            valid_rows = offset + jnp.arange(tile_rows, dtype=jnp.int32) < counts[expert_id]
            row_data = normed[row_ids // TOPK]
            output = expert_rows(row_data, expert_gate_weight[expert_id], expert_up_weight[expert_id], expert_down_weight[expert_id])
            weighted = jnp.where(valid_rows, flat_weight[row_ids], 0.0)[:, None] * output.astype(jnp.float32)
            return result_tile.at[row_ids // TOPK].add(weighted)
        return lax.fori_loop(jnp.int32(0), tile_count, per_tile, result_now)
    return lax.fori_loop(0, EXPERTS, per_expert, result)

def reference(query, forget_preact, value_input, output_gate, forget_minimum, extra_log_decay, head_norm_gain, output_weight, stream, feedforward_gain, routes, router_weight, expert_gate_weight, expert_up_weight, expert_down_weight):
    query_activated, incoming_weight, decay_logarithm = gate_factors(query, forget_preact, forget_minimum, extra_log_decay)
    value_rows = value_input.astype(jnp.float32)
    blocks = (head_blocks(query_activated, HEADS), head_blocks(incoming_weight, HEADS), head_blocks(value_rows, HEADS), head_blocks(decay_logarithm, HEADS))
    start_state = jnp.zeros((HEADS, STATE_ROW_COUNT, VALUE_CHANNELS), jnp.float32)
    _, block_outs = lax.scan(block_step, start_state, blocks)
    mixed = block_outs.transpose(0, 2, 1, 3).reshape(SEQUENCE_TOKENS, HEADS, VALUE_CHANNELS)
    hidden = head_output(mixed, head_norm_gain, output_gate)
    mix_rows = jnp.dot(hidden, output_weight, preferred_element_type=jnp.float32).astype(jnp.bfloat16)
    mix_rows = lax.optimization_barrier(mix_rows)
    residual = stream.astype(jnp.float32) + mix_rows.astype(jnp.float32)
    normed = rms_norm(residual, feedforward_gain)
    route_weight = router_weight / lax.optimization_barrier(jnp.sum(router_weight, axis=1, keepdims=True))
    routed_sum = routed(normed, routes, route_weight, expert_gate_weight, expert_up_weight, expert_down_weight)
    return (residual + routed_sum).astype(jnp.bfloat16)
```

```python
import functools

import jax
import jax.numpy as jnp
from jax import lax
from jax.experimental import pallas as pl
from jax.experimental.pallas import tpu as pltpu
from jax.sharding import PartitionSpec as P

TOPK = 2
EPSILON = 1e-06
OWNERS = 48
MESH = pl.DeviceIdType.MESH
f32 = jnp.float32
bf16 = jnp.bfloat16


def nn(a, b):
    return jnp.dot(a, b, preferred_element_type=f32)


def nt(a, b):
    return lax.dot_general(a, b, (((1,), (1,)), ((), ())), preferred_element_type=f32)


def tn(a, b):
    return lax.dot_general(a, b, (((0,), (0,)), ((), ())), preferred_element_type=f32)


def split2(x):
    hi = x.astype(bf16)
    return hi, (x - hi.astype(f32)).astype(bf16)


def split3(x):
    hi = x.astype(bf16)
    rest = x - hi.astype(f32)
    mid = rest.astype(bf16)
    return hi, mid, (rest - mid.astype(f32)).astype(bf16)


def sigmoid(x):
    return 1.0 / (1.0 + jnp.exp(-x))


def silu(x):
    return x / (1.0 + jnp.exp(-x))


def copy_to(src, dst, send, recv, target):
    return pltpu.make_async_remote_copy(
        src_ref=src, dst_ref=dst, send_sem=send, recv_sem=recv, device_id=target, device_id_type=MESH
    )


def wait_bytes(ref, sem):
    pltpu.make_async_copy(ref, ref, sem).wait()


def mixer_kernel(
    q_ref, f_ref, v_ref, g_ref, fmin_ref, eld_ref, gain_ref, wout_hbm, stream_hbm, ffgain_ref,
    normed_ref, resid_ref,
    wout, strm, msg, got, carr, back, acc, qe_hi, qe_lo, hid, ss,
    wsem, msend, mrecv, bsend, brecv, hsend, hrecv, ssend, srecv, tsend, trecv, lsem,
):
    rows = q_ref.shape[0]
    half = rows // 2
    heads = q_ref.shape[1] // 128
    me = lax.axis_index("sp")
    t = lax.axis_index("tp")
    n_sp = lax.axis_size("sp")
    n_tp = lax.axis_size("tp")
    right, left = lax.rem(t + 1, n_tp), lax.rem(t + n_tp - 1, n_tp)
    opposite = lax.rem(t + 2, n_tp)
    dcols = normed_ref.shape[1]
    quarter = rows // n_tp
    width = q_ref.shape[1]

    barrier = pltpu.get_barrier_semaphore()

    @pl.loop(1, n_sp)
    def _(k):
        pl.semaphore_signal(barrier, inc=1, device_id={"sp": lax.rem(me + k, n_sp)}, device_id_type=MESH)

    for k in range(1, n_tp):
        pl.semaphore_signal(barrier, inc=1, device_id={"tp": lax.rem(t + k, n_tp)}, device_id_type=MESH)

    weight_copy = pltpu.make_async_copy(wout_hbm, wout, wsem)
    weight_copy.start()
    own_rows = pl.ds(pl.multiple_of(t * quarter, quarter), quarter)
    own_stream = pltpu.make_async_copy(
        stream_hbm.at[:, pl.ds(pl.multiple_of(t * dcols, dcols), dcols)], strm.at[own_rows], lsem
    )
    own_stream.start()

    lower = (
        lax.broadcasted_iota(jnp.int32, (rows, rows), 0) >= lax.broadcasted_iota(jnp.int32, (rows, rows), 1)
    ).astype(bf16)
    weight = (1.0 - fmin_ref[...]) * sigmoid(-f_ref[...].astype(f32))
    d_hi, d_mid, d_lo = split3(jnp.log1p(-weight))
    decay = nn(lower, d_hi) + nn(lower, d_mid) + nn(lower, d_lo)
    e_hi, e_mid, e_lo = split3(eld_ref[...])
    extra = nt(lower, e_hi) + nt(lower, e_mid) + nt(lower, e_lo)

    row_of = lax.broadcasted_iota(jnp.int32, (8, 128), 0)
    parts = []
    for h in range(heads):
        lanes = slice(h * 128, (h + 1) * 128)
        run = decay[:, lanes] + extra[:, h : h + 1]
        w_h = weight[:, lanes]
        mid, end = run[half - 1 : half], run[rows - 1 : rows]
        v0, v1 = v_ref[0:half, lanes], v_ref[half:rows, lanes]
        k0_hi, k0_lo = split2(w_h[0:half] * jnp.exp(mid - run[0:half]))
        k1_hi, k1_lo = split2(w_h[half:rows] * jnp.exp(end - run[half:rows]))
        s0 = tn(v0, k0_hi) + tn(v0, k0_lo)
        s1 = tn(v1, k1_hi) + tn(v1, k1_lo)
        local = jnp.exp(end - mid) * s0 + s1
        t_hi, t_mid, t_lo = split3(end)
        tail = jnp.where(
            row_of == 0,
            t_hi.astype(f32),
            jnp.where(row_of == 1, t_mid.astype(f32), jnp.where(row_of == 2, t_lo.astype(f32), 0.0)),
        )
        piece = jnp.concatenate(
            [local.reshape(16, 8, 128), jnp.broadcast_to(tail[None], (16, 8, 128))], axis=1
        )
        msg[h * 16 : (h + 1) * 16] = piece.astype(bf16)
        parts.append((run, w_h, v0, v1, mid, s0))

    pl.semaphore_wait(barrier, n_sp + n_tp - 2)

    def owner_device(p):
        return (p // 3) * 4 + lax.rem(p, 3)

    is_owner = lax.rem(me, 4) < 3
    mine = (me // 4) * 3 + jnp.minimum(lax.rem(me, 4), 2)

    @pl.loop(0, OWNERS)
    def _(k):
        p = lax.rem(mine + k, OWNERS)
        target = owner_device(p)

        @pl.when(target != me)
        def _():
            copy_to(msg.at[p], got.at[me], msend, mrecv, {"sp": target}).start()

    for k in range(1, n_tp):
        other = lax.rem(t + k, n_tp)
        copy_to(
            stream_hbm.at[:, pl.ds(pl.multiple_of(other * dcols, dcols), dcols)],
            strm.at[own_rows],
            tsend.at[k - 1],
            trecv.at[k - 1],
            {"tp": other},
        ).start()

    causal = lax.broadcasted_iota(jnp.int32, (half, half), 0) >= lax.broadcasted_iota(
        jnp.int32, (half, half), 1
    )
    for h in range(heads):
        lanes = slice(h * 128, (h + 1) * 128)
        run, w_h, v0, v1, mid, s0 = parts[h]
        query = silu(q_ref[:, lanes].astype(f32))
        full_hi, full_lo = split2(query * jnp.exp(run))
        qe_hi[:, lanes] = full_hi
        qe_lo[:, lanes] = full_lo
        for c, values in ((0, v0), (1, v1)):
            span = slice(c * half, (c + 1) * half)
            centre = run[c * half + half // 2 - 1 : c * half + half // 2]
            a_hi, a_lo = split2(query[span] * jnp.exp(run[span] - centre))
            b_hi, b_lo = split2(w_h[span] * jnp.exp(centre - run[span]))
            scores = nt(a_hi, b_hi) + nt(a_hi, b_lo) + nt(a_lo, b_hi)
            p_hi, p_lo = split2(jnp.where(causal, scores, 0.0))
            out = nn(p_hi, values) + nn(p_lo, values)
            if c == 1:
                c_hi, c_lo = split2(query[span] * jnp.exp(run[span] - mid))
                z_hi, z_lo = split2(s0)
                out = out + nt(c_hi, z_hi) + nt(c_hi, z_lo) + nt(c_lo, z_hi)
            acc[span, lanes] = out

    @pl.when(is_owner)
    def _():
        got[me] = msg[mine]
        wait_bytes(got.at[pl.ds(0, n_sp - 1)], mrecv)

        def step(i, state):
            carr[i] = state.astype(bf16)
            block = got[i].astype(f32)
            total = block[8:9] + block[9:10] + block[10:11]
            return jnp.exp(total) * state + block[0:8]

        lax.fori_loop(0, n_sp, step, jnp.zeros((8, 128), f32), unroll=8)
        back[mine] = carr[me]

        @pl.loop(1, n_sp)
        def _(k):
            target = lax.rem(me + k, n_sp)
            copy_to(carr.at[target], back.at[mine], bsend, brecv, {"sp": target}).start()

    gate = gain_ref[...] * silu(g_ref[...].astype(f32))

    @pl.when(is_owner)
    def _():
        wait_bytes(back.at[pl.ds(0, OWNERS - 1)], brecv)

    @pl.when(jnp.logical_not(is_owner))
    def _():
        wait_bytes(back.at[pl.ds(0, OWNERS)], brecv)

    for h in range(heads):
        lanes = slice(h * 128, (h + 1) * 128)
        state = back[h * 16 : (h + 1) * 16].astype(f32).reshape(128, 128).astype(bf16)
        out = acc[:, lanes] + nt(qe_hi[:, lanes], state) + nt(qe_lo[:, lanes], state)
        out = out * lax.rsqrt(jnp.mean(out * out, axis=1, keepdims=True) + EPSILON)
        hid[t, :, lanes] = (out * gate[:, lanes]).astype(bf16)

    top, low = pl.ds(0, half), pl.ds(half, half)
    to_right = [
        copy_to(hid.at[t, r], hid.at[t, r], hsend.at[i], hrecv.at[i], {"tp": right})
        for i, r in enumerate((top, low))
    ]
    to_left = [
        copy_to(hid.at[t, r], hid.at[t, r], hsend.at[2 + i], hrecv.at[2 + i], {"tp": left})
        for i, r in enumerate((low, top))
    ]
    to_right[0].start()
    to_left[0].start()
    to_right[1].start()
    to_left[1].start()
    weight_copy.wait()

    def partial(block):
        return nn(hid[block], wout[pl.ds(pl.multiple_of(block * width, width), width), :])

    proj = partial(t)
    to_right[0].wait_recv()
    on_right = copy_to(hid.at[left, top], hid.at[left, top], hsend.at[4], hrecv.at[4], {"tp": right})
    on_right.start()
    to_left[0].wait_recv()
    on_left = copy_to(hid.at[right, low], hid.at[right, low], hsend.at[5], hrecv.at[5], {"tp": left})
    on_left.start()
    to_right[1].wait_recv()
    proj = proj + partial(left)
    to_left[1].wait_recv()
    proj = proj + partial(right)
    own_stream.wait()
    for k in range(1, n_tp):
        other = lax.rem(t + k, n_tp)
        copy_to(
            stream_hbm.at[:, pl.ds(pl.multiple_of(other * dcols, dcols), dcols)],
            strm.at[own_rows],
            tsend.at[k - 1],
            trecv.at[k - 1],
            {"tp": other},
        ).wait()
    on_right.wait_recv()
    on_left.wait_recv()
    proj = proj + partial(opposite)
    resid = strm[...].astype(f32) + proj.astype(bf16).astype(f32)
    resid_ref[...] = resid
    r_hi, r_mid, r_lo = split3(resid * resid)
    ones = jnp.ones((8, dcols), bf16)
    ss[t] = nt(ones, r_hi) + nt(ones, r_mid) + nt(ones, r_lo)
    sums = []
    for k in range(1, n_tp):
        sums.append(
            copy_to(ss.at[t], ss.at[t], ssend.at[k - 1], srecv.at[k - 1], {"tp": lax.rem(t + k, n_tp)})
        )
        sums[-1].start()
    for c in sums:
        c.wait_recv()
    total = ss[0]
    for k in range(1, n_tp):
        total = total + ss[k]
    scale = lax.rsqrt(total / (n_tp * dcols) + EPSILON)
    unit = (
        lax.broadcasted_iota(jnp.int32, (rows, rows), 0) == lax.broadcasted_iota(jnp.int32, (rows, rows), 1)
    ).astype(bf16)
    i_hi, i_mid, i_lo = split3(scale)
    column = (nt(unit, i_hi) + nt(unit, i_mid) + nt(unit, i_lo))[:, 0:1]
    normed_ref[...] = (resid_ref[...] * column * ffgain_ref[t]).astype(bf16)

    for c in sums + to_right + to_left + [on_right, on_left]:
        c.wait_send()

    @pl.when(is_owner)
    def _():
        wait_bytes(msg.at[pl.ds(0, OWNERS - 1)], msend)
        wait_bytes(carr.at[pl.ds(0, n_sp - 1)], bsend)

    @pl.when(jnp.logical_not(is_owner))
    def _():
        wait_bytes(msg.at[pl.ds(0, OWNERS)], msend)


def mixer(query, forget, value, gate, fmin, eld, gain, wout, stream, ffgain):
    rows, width = query.shape
    n_sp, n_tp = lax.axis_size("sp"), lax.axis_size("tp")
    model = stream.shape[1]
    dcols = model // n_tp
    vmem = pl.BlockSpec(memory_space=pltpu.VMEM)
    hbm = pl.BlockSpec(memory_space=pl.ANY)
    dma = pltpu.SemaphoreType.DMA
    return pl.pallas_call(
        mixer_kernel,
        name="mixer",
        out_shape=(
            jax.ShapeDtypeStruct((rows, dcols), bf16),
            jax.ShapeDtypeStruct((rows, dcols), f32),
        ),
        in_specs=[vmem] * 7 + [hbm, hbm, vmem],
        out_specs=(vmem, vmem),
        scratch_shapes=[
            pltpu.VMEM(wout.shape, bf16),
            pltpu.VMEM((rows, dcols), bf16),
            pltpu.VMEM((OWNERS, 16, 128), bf16),
            pltpu.VMEM((n_sp, 16, 128), bf16),
            pltpu.VMEM((n_sp, 8, 128), bf16),
            pltpu.VMEM((OWNERS, 8, 128), bf16),
            pltpu.VMEM((rows, width), f32),
            pltpu.VMEM((rows, width), bf16),
            pltpu.VMEM((rows, width), bf16),
            pltpu.VMEM((n_tp, rows, width), bf16),
            pltpu.VMEM((n_tp, 8, rows), f32),
            dma,
            dma,
            dma,
            dma,
            dma,
            dma((6,)),
            dma((6,)),
            dma((3,)),
            dma((3,)),
            dma((3,)),
            dma((3,)),
            dma,
        ],
        compiler_params=pltpu.CompilerParams(
            collective_id=0, has_side_effects=True, vmem_limit_bytes=40 * 2**20
        ),
    )(
        query, forget, value, gate, fmin[None], eld, gain[None], wout, stream,
        ffgain.reshape(n_tp, 1, dcols),
    )


def per_device(
    query, forget_preact, value_input, output_gate, forget_minimum, extra_log_decay, head_norm_gain,
    output_weight, stream, feedforward_gain, routes, router_weight,
    expert_gate_weight, expert_up_weight, expert_down_weight,
):
    rows = query.shape[0]
    n_sp, n_tp = lax.axis_size("sp"), lax.axis_size("tp")
    normed, resid = mixer(
        query, forget_preact, value_input, output_gate, forget_minimum, extra_log_decay,
        head_norm_gain, output_weight, stream, feedforward_gain,
    )
    dcols = normed.shape[1]
    quarter = rows // n_tp
    capacity = quarter * n_tp // n_sp
    picks = routes.reshape(n_tp, quarter * TOPK)
    onehot = (picks[:, :, None] == jnp.arange(n_sp, dtype=jnp.int32)).astype(jnp.int32)
    rank = jnp.sum((jnp.cumsum(onehot, axis=1) - 1) * onehot, axis=2)
    block = jnp.arange(n_tp, dtype=jnp.int32)[:, None]
    slots = ((picks * n_tp + block) * capacity + rank).reshape(rows, TOPK)
    grid = jnp.arange(n_sp * n_tp * capacity, dtype=jnp.int32)
    table = jnp.sum((slots[:, :, None] == grid).astype(bf16), axis=1)
    sendbuf = tn(table, normed).astype(bf16)
    received = lax.all_to_all(
        sendbuf.reshape(n_sp, n_tp * capacity, dcols), "sp", split_axis=0, concat_axis=0, tiled=True
    ).reshape(-1, dcols)
    arrived = lax.all_gather(received, "tp", axis=0)
    gate_w = expert_gate_weight[0].reshape(n_tp, dcols, -1)
    up_w = expert_up_weight[0].reshape(n_tp, dcols, -1)
    gate_act = sum(nn(arrived[k], gate_w[k]) for k in range(n_tp))
    up_act = sum(nn(arrived[k], up_w[k]) for k in range(n_tp))
    inner = (silu(gate_act) * up_act).astype(bf16)
    inner = lax.all_gather(inner, "tp", axis=1, tiled=True)
    down = lax.all_to_all(expert_down_weight[0], "tp", split_axis=1, concat_axis=0, tiled=True)
    outs = nn(inner, down).astype(bf16)
    returned = lax.all_to_all(
        outs.reshape(n_sp, n_tp * capacity, dcols), "sp", split_axis=0, concat_axis=0, tiled=True
    ).reshape(-1, dcols)
    weights = lax.all_gather(
        router_weight / jnp.sum(router_weight, axis=1, keepdims=True), "tp", axis=0, tiled=True
    )
    routed = sum(
        weights[:, j : j + 1] * nn((slots[:, j : j + 1] == grid).astype(bf16), returned)
        for j in range(TOPK)
    )
    result = (resid + routed).astype(bf16)
    return lax.all_to_all(result, "tp", split_axis=0, concat_axis=1, tiled=True)


def solution(mesh):
    both = ("sp", "tp")
    placed = (
        P("sp", "tp"), P("sp", "tp"), P("sp", "tp"), P("sp", "tp"), P("tp"), P("tp", "sp"), P("tp"),
        P(None, "tp"), P(both, None), P(), P("sp", None), P(both, None),
        P("sp", None, "tp"), P("sp", None, "tp"), P("sp", "tp", None),
    )
    return jax.shard_map(
        per_device, mesh=mesh, in_specs=placed, out_specs=P(both, None), check_vma=False
    )
```

```python
import jax
import jax.numpy as jnp
from jax import lax
from jax.experimental import pallas as pl
from jax.experimental.pallas import tpu as pltpu
from jax.sharding import PartitionSpec as P

TOPK = 2
EPSILON = 1e-06
OWNERS = 48
MESH = pl.DeviceIdType.MESH
f32 = jnp.float32
bf16 = jnp.bfloat16


def nn(a, b):
    return jnp.dot(a, b, preferred_element_type=f32)


def nt(a, b):
    return lax.dot_general(a, b, (((1,), (1,)), ((), ())), preferred_element_type=f32)


def tn(a, b):
    return lax.dot_general(a, b, (((0,), (0,)), ((), ())), preferred_element_type=f32)


def split2(x):
    hi = x.astype(bf16)
    return hi, (x - hi.astype(f32)).astype(bf16)


def split3(x):
    hi = x.astype(bf16)
    rest = x - hi.astype(f32)
    mid = rest.astype(bf16)
    return hi, mid, (rest - mid.astype(f32)).astype(bf16)


def sigmoid(x):
    return 1.0 / (1.0 + jnp.exp(-x))


def silu(x):
    return x / (1.0 + jnp.exp(-x))


def copy_to(src, dst, send, recv, target):
    return pltpu.make_async_remote_copy(
        src_ref=src, dst_ref=dst, send_sem=send, recv_sem=recv, device_id=target, device_id_type=MESH
    )


def wait_bytes(ref, sem):
    pltpu.make_async_copy(ref, ref, sem).wait()


def layer_kernel(
    q_ref, f_ref, v_ref, g_ref, fmin_ref, eld_ref, gain_ref, wout_hbm, stream_hbm, ffgain_ref,
    routes_ref, router_ref, gate_hbm, up_hbm, down_hbm,
    out_ref,
    wout, strm, msg, got, carr, back, acc, qe_hi, qe_lo, hid, ss, resid_ref,
    gate_w, up_w, down_w, to_slots, from_slots, router, sendbuf, rows_in, inner, outs, returned, slices, final,
    wsem, msend, mrecv, bsend, brecv, hsend, hrecv, ssend, srecv, tsend, trecv, lsem,
    gsem, usem, dsem, dsend, drecv, psend, precv, zsend, zrecv, xsend, xrecv, isend, irecv,
    rsend, rrecv, fsend, frecv,
):
    rows = q_ref.shape[0]
    half = rows // 2
    heads = q_ref.shape[1] // 128
    me = lax.axis_index("sp")
    t = lax.axis_index("tp")
    n_sp = lax.axis_size("sp")
    n_tp = lax.axis_size("tp")
    right, left = lax.rem(t + 1, n_tp), lax.rem(t + n_tp - 1, n_tp)
    opposite = lax.rem(t + 2, n_tp)
    dcols = resid_ref.shape[1]
    quarter = rows // n_tp
    width = q_ref.shape[1]

    barrier = pltpu.get_barrier_semaphore()

    @pl.loop(1, n_sp)
    def _(k):
        pl.semaphore_signal(barrier, inc=1, device_id={"sp": lax.rem(me + k, n_sp)}, device_id_type=MESH)

    for k in range(1, n_tp):
        pl.semaphore_signal(barrier, inc=1, device_id={"tp": lax.rem(t + k, n_tp)}, device_id_type=MESH)

    weight_copy = pltpu.make_async_copy(wout_hbm, wout, wsem)
    weight_copy.start()
    own_rows = pl.ds(pl.multiple_of(t * quarter, quarter), quarter)
    own_stream = pltpu.make_async_copy(
        stream_hbm.at[:, pl.ds(pl.multiple_of(t * dcols, dcols), dcols)], strm.at[own_rows], lsem
    )
    own_stream.start()
    gate_copy = pltpu.make_async_copy(gate_hbm.at[0], gate_w, gsem)
    up_copy = pltpu.make_async_copy(up_hbm.at[0], up_w, usem)
    gate_copy.start()
    up_copy.start()
    hidden_units = down_hbm.shape[1]
    own_units = pl.ds(pl.multiple_of(t * hidden_units, hidden_units), hidden_units)

    def down_part(k):
        return down_hbm.at[0, :, pl.ds(pl.multiple_of(k * dcols, dcols), dcols)]

    own_down = pltpu.make_async_copy(down_part(t), down_w.at[own_units], dsem)
    own_down.start()
    picked = router_ref[...] / (router_ref[0:1] + router_ref[1:2])
    router[t] = jnp.zeros((8, 128), f32)
    router[t, 0:TOPK, 0:quarter] = picked

    lower = (
        lax.broadcasted_iota(jnp.int32, (rows, rows), 0) >= lax.broadcasted_iota(jnp.int32, (rows, rows), 1)
    ).astype(bf16)
    weight = (1.0 - fmin_ref[...]) * sigmoid(-f_ref[...].astype(f32))
    d_hi, d_mid, d_lo = split3(jnp.log1p(-weight))
    decay = nn(lower, d_hi) + nn(lower, d_mid) + nn(lower, d_lo)
    e_hi, e_mid, e_lo = split3(eld_ref[...])
    extra = nt(lower, e_hi) + nt(lower, e_mid) + nt(lower, e_lo)

    row_of = lax.broadcasted_iota(jnp.int32, (8, 128), 0)
    parts = []
    for h in range(heads):
        lanes = slice(h * 128, (h + 1) * 128)
        run = decay[:, lanes] + extra[:, h : h + 1]
        w_h = weight[:, lanes]
        mid, end = run[half - 1 : half], run[rows - 1 : rows]
        v0, v1 = v_ref[0:half, lanes], v_ref[half:rows, lanes]
        k0_hi, k0_lo = split2(w_h[0:half] * jnp.exp(mid - run[0:half]))
        k1_hi, k1_lo = split2(w_h[half:rows] * jnp.exp(end - run[half:rows]))
        s0 = tn(v0, k0_hi) + tn(v0, k0_lo)
        s1 = tn(v1, k1_hi) + tn(v1, k1_lo)
        local = jnp.exp(end - mid) * s0 + s1
        t_hi, t_mid, t_lo = split3(end)
        tail = jnp.where(
            row_of == 0,
            t_hi.astype(f32),
            jnp.where(row_of == 1, t_mid.astype(f32), jnp.where(row_of == 2, t_lo.astype(f32), 0.0)),
        )
        piece = jnp.concatenate(
            [local.reshape(16, 8, 128), jnp.broadcast_to(tail[None], (16, 8, 128))], axis=1
        )
        msg[h * 16 : (h + 1) * 16] = piece.astype(bf16)
        parts.append((run, w_h, v0, v1, mid, s0))

    pl.semaphore_wait(barrier, n_sp + n_tp - 2)

    def owner_device(p):
        return (p // 3) * 4 + lax.rem(p, 3)

    is_owner = lax.rem(me, 4) < 3
    mine = (me // 4) * 3 + jnp.minimum(lax.rem(me, 4), 2)

    @pl.loop(0, OWNERS)
    def _(k):
        p = lax.rem(mine + k, OWNERS)
        target = owner_device(p)

        @pl.when(target != me)
        def _():
            copy_to(msg.at[p], got.at[me], msend, mrecv, {"sp": target}).start()

    for k in range(1, n_tp):
        other = lax.rem(t + k, n_tp)
        copy_to(
            stream_hbm.at[:, pl.ds(pl.multiple_of(other * dcols, dcols), dcols)],
            strm.at[own_rows],
            tsend.at[k - 1],
            trecv.at[k - 1],
            {"tp": other},
        ).start()
    shares = [
        copy_to(router.at[t], router.at[t], psend.at[k - 1], precv.at[k - 1], {"tp": lax.rem(t + k, n_tp)})
        for k in range(1, n_tp)
    ]
    for c in shares:
        c.start()
    down_sends = [
        copy_to(down_part(other), down_w.at[own_units], dsend.at[k], drecv.at[k], {"tp": other})
        for k, other in enumerate((right, left, opposite))
    ]
    down_sends[0].start()
    down_sends[1].start()

    slots = n_sp * 16
    unit = (
        lax.broadcasted_iota(jnp.int32, (rows, rows), 0) == lax.broadcasted_iota(jnp.int32, (rows, rows), 1)
    ).astype(bf16)
    first = lax.broadcasted_iota(jnp.int32, (rows, rows), 0)
    second = lax.broadcasted_iota(jnp.int32, (rows, rows), 1)
    same = (first >> 6) == (second >> 6)
    earlier = ((first < second) & same).astype(bf16)
    later = ((second < first) & same).astype(bf16)
    routes = routes_ref[...]
    slot = lax.broadcasted_iota(jnp.int32, (slots, rows), 0)
    token = lax.broadcasted_iota(jnp.int32, (slots, rows), 1)
    named = (routes[0:1] == (slot >> 4)) | (routes[1:2] == (slot >> 4))
    count = nn(named.astype(bf16), earlier)
    here = named & (count == (slot & 3).astype(f32)) & (((slot >> 2) & 3) == (token >> 6))
    to_slots[...] = here.astype(bf16)
    columns = nt(unit, routes.astype(f32).astype(bf16))
    slot = lax.broadcasted_iota(jnp.int32, (rows, slots), 1)
    token = lax.broadcasted_iota(jnp.int32, (rows, slots), 0)
    expert = (slot >> 4).astype(f32)
    chosen = [columns[:, j : j + 1] == expert for j in range(TOPK)]
    count = nn(later, (chosen[0] | chosen[1]).astype(bf16))
    fits = (count == (slot & 3).astype(f32)) & (((slot >> 2) & 3) == (token >> 6))
    for j in range(TOPK):
        from_slots[j] = (chosen[j] & fits).astype(bf16)

    causal = lax.broadcasted_iota(jnp.int32, (half, half), 0) >= lax.broadcasted_iota(
        jnp.int32, (half, half), 1
    )
    for h in range(heads):
        lanes = slice(h * 128, (h + 1) * 128)
        run, w_h, v0, v1, mid, s0 = parts[h]
        query = silu(q_ref[:, lanes].astype(f32))
        full_hi, full_lo = split2(query * jnp.exp(run))
        qe_hi[:, lanes] = full_hi
        qe_lo[:, lanes] = full_lo
        for c, values in ((0, v0), (1, v1)):
            span = slice(c * half, (c + 1) * half)
            centre = run[c * half + half // 2 - 1 : c * half + half // 2]
            a_hi, a_lo = split2(query[span] * jnp.exp(run[span] - centre))
            b_hi, b_lo = split2(w_h[span] * jnp.exp(centre - run[span]))
            scores = nt(a_hi, b_hi) + nt(a_hi, b_lo) + nt(a_lo, b_hi)
            p_hi, p_lo = split2(jnp.where(causal, scores, 0.0))
            out = nn(p_hi, values) + nn(p_lo, values)
            if c == 1:
                c_hi, c_lo = split2(query[span] * jnp.exp(run[span] - mid))
                z_hi, z_lo = split2(s0)
                out = out + nt(c_hi, z_hi) + nt(c_hi, z_lo) + nt(c_lo, z_hi)
            acc[span, lanes] = out

    @pl.when(is_owner)
    def _():
        got[me] = msg[mine]
        wait_bytes(got.at[pl.ds(0, n_sp - 1)], mrecv)

        def step(i, state):
            carr[i] = state.astype(bf16)
            block = got[i].astype(f32)
            total = block[8:9] + block[9:10] + block[10:11]
            return jnp.exp(total) * state + block[0:8]

        lax.fori_loop(0, n_sp, step, jnp.zeros((8, 128), f32), unroll=8)
        back[mine] = carr[me]

        @pl.loop(1, n_sp)
        def _(k):
            target = lax.rem(me + k, n_sp)
            copy_to(carr.at[target], back.at[mine], bsend, brecv, {"sp": target}).start()

    gate = gain_ref[...] * silu(g_ref[...].astype(f32))

    @pl.when(is_owner)
    def _():
        wait_bytes(back.at[pl.ds(0, OWNERS - 1)], brecv)

    @pl.when(jnp.logical_not(is_owner))
    def _():
        wait_bytes(back.at[pl.ds(0, OWNERS)], brecv)

    for h in range(heads):
        lanes = slice(h * 128, (h + 1) * 128)
        state = back[h * 16 : (h + 1) * 16].astype(f32).reshape(128, 128).astype(bf16)
        out = acc[:, lanes] + nt(qe_hi[:, lanes], state) + nt(qe_lo[:, lanes], state)
        out = out * lax.rsqrt(jnp.mean(out * out, axis=1, keepdims=True) + EPSILON)
        hid[t, :, lanes] = (out * gate[:, lanes]).astype(bf16)

    top, low = pl.ds(0, half), pl.ds(half, half)
    to_right = [
        copy_to(hid.at[t, r], hid.at[t, r], hsend.at[i], hrecv.at[i], {"tp": right})
        for i, r in enumerate((top, low))
    ]
    to_left = [
        copy_to(hid.at[t, r], hid.at[t, r], hsend.at[2 + i], hrecv.at[2 + i], {"tp": left})
        for i, r in enumerate((low, top))
    ]
    to_right[0].start()
    to_left[0].start()
    to_right[1].start()
    to_left[1].start()
    weight_copy.wait()

    def partial(block):
        return nn(hid[block], wout[pl.ds(pl.multiple_of(block * width, width), width), :])

    proj = partial(t)
    to_right[0].wait_recv()
    on_right = copy_to(hid.at[left, top], hid.at[left, top], hsend.at[4], hrecv.at[4], {"tp": right})
    on_right.start()
    to_left[0].wait_recv()
    on_left = copy_to(hid.at[right, low], hid.at[right, low], hsend.at[5], hrecv.at[5], {"tp": left})
    on_left.start()
    to_right[1].wait_recv()
    proj = proj + partial(left)
    to_left[1].wait_recv()
    proj = proj + partial(right)
    own_stream.wait()
    for k in range(1, n_tp):
        other = lax.rem(t + k, n_tp)
        copy_to(
            stream_hbm.at[:, pl.ds(pl.multiple_of(other * dcols, dcols), dcols)],
            strm.at[own_rows],
            tsend.at[k - 1],
            trecv.at[k - 1],
            {"tp": other},
        ).wait()
    on_right.wait_recv()
    on_left.wait_recv()
    down_sends[2].start()
    proj = proj + partial(opposite)
    resid = strm[...].astype(f32) + proj.astype(bf16).astype(f32)
    resid_ref[...] = resid
    r_hi, r_mid, r_lo = split3(resid * resid)
    ones = jnp.ones((8, dcols), bf16)
    ss[t] = nt(ones, r_hi) + nt(ones, r_mid) + nt(ones, r_lo)
    sums = []
    for k in range(1, n_tp):
        sums.append(
            copy_to(ss.at[t], ss.at[t], ssend.at[k - 1], srecv.at[k - 1], {"tp": lax.rem(t + k, n_tp)})
        )
        sums[-1].start()
    for c in sums:
        c.wait_recv()
    total = ss[0]
    for k in range(1, n_tp):
        total = total + ss[k]
    scale = lax.rsqrt(total / (n_tp * dcols) + EPSILON)
    i_hi, i_mid, i_lo = split3(scale)
    column = (nt(unit, i_hi) + nt(unit, i_mid) + nt(unit, i_lo))[:, 0:1]
    normed = (resid_ref[...] * column * ffgain_ref[t]).astype(bf16)
    sendbuf[...] = nn(to_slots[...], normed).astype(bf16)

    plane_size = 8
    planes = n_sp // plane_size
    z = me // plane_size
    b_me = lax.rem(me, plane_size)
    span, part = plane_size * 16, plane_size * 8

    def message(k):
        return pl.ds(pl.multiple_of(k * 16, 16), 16)

    def chunk(i):
        return lax.rem(z + i, planes) * span

    def whole(i):
        return pl.ds(pl.multiple_of(chunk(i), span), span)

    def piece(i, s):
        return pl.ds(pl.multiple_of(chunk(i) + s * part, part), part)

    @pl.loop(1, plane_size)
    def _(k):
        target = z * plane_size + lax.rem(b_me + k, plane_size)
        copy_to(
            sendbuf.at[message(target)], rows_in.at[t, message(me)], zsend, zrecv.at[0], {"sp": target}
        ).start()

    for i in (1, 4, 2, 5, 3, 6, 7):

        @pl.loop(0, plane_size)
        def _(k, i=i):
            target = lax.rem(z + planes - i, planes) * plane_size + lax.rem(b_me + k, plane_size)
            copy_to(
                sendbuf.at[message(target)], rows_in.at[t, message(me)], zsend, zrecv.at[i], {"sp": target}
            ).start()

    rows_in[t, message(me)] = sendbuf[message(me)]
    gate_copy.wait()
    up_copy.wait()

    def ring_start(ref, i, send, recv):
        for s, target, n in ((0, right, 0), (1, left, 2), (1, right, 1), (0, left, 3)):
            here = ref.at[t, piece(i, s)]
            copy_to(here, here, send, recv.at[i, n], {"tp": target}).start()

    def ring_forward(ref, i, send, recv):
        for s, source, target, n in ((0, left, right, 0), (1, right, left, 2)):
            here = ref.at[source, piece(i, s)]
            wait_bytes(here, recv.at[i, n])
            copy_to(here, here, send, recv.at[i, 4 + s], {"tp": target}).start()

    def ring_end(ref, i, recv):
        wait_bytes(ref.at[left, piece(i, 1)], recv.at[i, 1])
        wait_bytes(ref.at[right, piece(i, 0)], recv.at[i, 3])
        wait_bytes(ref.at[opposite, piece(i, 0)], recv.at[i, 4])
        wait_bytes(ref.at[opposite, piece(i, 1)], recv.at[i, 5])

    @pl.loop(0, planes + 4)
    def _(i):
        @pl.when(i == 0)
        def _():
            wait_bytes(rows_in.at[t, pl.ds(0, span - 16)], zrecv.at[0])
            ring_start(rows_in, 0, xsend, xrecv)

        @pl.when((i > 0) & (i < planes))
        def _():
            wait_bytes(rows_in.at[t, whole(i)], zrecv.at[i])
            ring_start(rows_in, i, xsend, xrecv)

        @pl.when((i >= 1) & (i < planes + 1))
        def _():
            ring_forward(rows_in, i - 1, xsend, xrecv)

        @pl.when((i >= 2) & (i < planes + 2))
        def _():
            j = i - 2
            ring_end(rows_in, j, xrecv)
            gate_act = jnp.zeros((span, gate_w.shape[1]), f32)
            up_act = jnp.zeros((span, gate_w.shape[1]), f32)
            for k in range(n_tp):
                block = rows_in[k, whole(j)]
                gate_act = gate_act + nn(block, gate_w[k * dcols : (k + 1) * dcols])
                up_act = up_act + nn(block, up_w[k * dcols : (k + 1) * dcols])
            inner[t, whole(j)] = (silu(gate_act) * up_act).astype(bf16)
            ring_start(inner, j, isend, irecv)

        @pl.when((i >= 3) & (i < planes + 3))
        def _():
            ring_forward(inner, i - 3, isend, irecv)

        @pl.when(i >= 4)
        def _():
            j = i - 4

            @pl.when(j == 0)
            def _():
                own_down.wait()
                for c in down_sends:
                    c.wait_recv()

            ring_end(inner, j, irecv)
            out = jnp.zeros((span, dcols), f32)
            for k in range(n_tp):
                out = out + nn(
                    inner[k, whole(j)], down_w[k * hidden_units : (k + 1) * hidden_units]
                )
            outs[whole(j)] = out.astype(bf16)

            @pl.loop(0, plane_size)
            def _(k):
                target = lax.rem(z + j, planes) * plane_size + lax.rem(b_me + k, plane_size)

                @pl.when(target != me)
                def _():
                    copy_to(
                        outs.at[message(target)], returned.at[message(me)], rsend, rrecv, {"sp": target}
                    ).start()

    returned[message(me)] = outs[message(me)]
    for c in shares:
        c.wait_recv()
    eye = (
        lax.broadcasted_iota(jnp.int32, (quarter, 128), 0) == lax.broadcasted_iota(jnp.int32, (quarter, 128), 1)
    ).astype(bf16)
    shares_of = []
    for k in range(n_tp):
        p_hi, p_mid, p_lo = split3(router[k])
        shares_of.append(nt(eye, p_hi) + nt(eye, p_mid) + nt(eye, p_lo))
    share = jnp.concatenate(shares_of, axis=0)
    wait_bytes(returned.at[pl.ds(0, slots - 16)], rrecv)
    total = resid_ref[...]
    for j in range(TOPK):
        total = total + share[:, j : j + 1] * nn(from_slots[j], returned[...])
    slices[...] = total.astype(bf16)
    own_cols = pl.ds(pl.multiple_of(t * dcols, dcols), dcols)
    last = []
    for k in range(1, n_tp):
        other = lax.rem(t + k, n_tp)
        last.append(
            copy_to(
                slices.at[pl.ds(pl.multiple_of(other * quarter, quarter), quarter)],
                final.at[:, own_cols],
                fsend.at[k - 1],
                frecv.at[k - 1],
                {"tp": other},
            )
        )
        last[-1].start()
    final[:, own_cols] = slices[own_rows]
    for c in last:
        c.wait_recv()
    out_ref[...] = final[...]
    for c in last + shares + down_sends:
        c.wait_send()
    wait_bytes(sendbuf.at[pl.ds(0, slots - 16)], zsend)
    wait_bytes(outs.at[pl.ds(0, slots - 16)], rsend)
    wait_bytes(rows_in.at[pl.ds(0, 3)], xsend)
    wait_bytes(inner.at[pl.ds(0, 3)], isend)
    for c in sums + to_right + to_left + [on_right, on_left]:
        c.wait_send()

    @pl.when(is_owner)
    def _():
        wait_bytes(msg.at[pl.ds(0, OWNERS - 1)], msend)
        wait_bytes(carr.at[pl.ds(0, n_sp - 1)], bsend)

    @pl.when(jnp.logical_not(is_owner))
    def _():
        wait_bytes(msg.at[pl.ds(0, OWNERS)], msend)


def per_device(
    query, forget, value, gate, fmin, eld, gain, wout, stream, ffgain, routes, router,
    gate_weight, up_weight, down_weight,
):
    rows, width = query.shape
    n_sp, n_tp = lax.axis_size("sp"), lax.axis_size("tp")
    model = stream.shape[1]
    dcols = model // n_tp
    slots = n_sp * 16
    units = down_weight.shape[1]
    vmem = pl.BlockSpec(memory_space=pltpu.VMEM)
    hbm = pl.BlockSpec(memory_space=pl.ANY)
    dma = pltpu.SemaphoreType.DMA
    return pl.pallas_call(
        layer_kernel,
        name="layer",
        out_shape=jax.ShapeDtypeStruct(stream.shape, bf16),
        in_specs=[vmem] * 7 + [hbm, hbm] + [vmem] * 3 + [hbm] * 3,
        out_specs=vmem,
        scratch_shapes=[
            pltpu.VMEM(wout.shape, bf16),
            pltpu.VMEM((rows, dcols), bf16),
            pltpu.VMEM((OWNERS, 16, 128), bf16),
            pltpu.VMEM((n_sp, 16, 128), bf16),
            pltpu.VMEM((n_sp, 8, 128), bf16),
            pltpu.VMEM((OWNERS, 8, 128), bf16),
            pltpu.VMEM((rows, width), f32),
            pltpu.VMEM((rows, width), bf16),
            pltpu.VMEM((rows, width), bf16),
            pltpu.VMEM((n_tp, rows, width), bf16),
            pltpu.VMEM((n_tp, 8, rows), f32),
            pltpu.VMEM((rows, dcols), f32),
            pltpu.VMEM((model, units), bf16),
            pltpu.VMEM((model, units), bf16),
            pltpu.VMEM((n_tp * units, dcols), bf16),
            pltpu.VMEM((slots, rows), bf16),
            pltpu.VMEM((TOPK, rows, slots), bf16),
            pltpu.VMEM((n_tp, 8, 128), f32),
            pltpu.VMEM((slots, dcols), bf16),
            pltpu.VMEM((n_tp, slots, dcols), bf16),
            pltpu.VMEM((n_tp, slots, units), bf16),
            pltpu.VMEM((slots, dcols), bf16),
            pltpu.VMEM((slots, dcols), bf16),
            pltpu.VMEM((rows, dcols), bf16),
            pltpu.VMEM(stream.shape, bf16),
            dma, dma, dma, dma, dma, dma((6,)), dma((6,)), dma((3,)), dma((3,)), dma((3,)), dma((3,)), dma,
            dma, dma, dma, dma((3,)), dma((3,)), dma((3,)), dma((3,)),
            dma, dma((8,)), dma, dma((8, 6)), dma, dma((8, 6)), dma, dma, dma((3,)), dma((3,)),
        ],
        compiler_params=pltpu.CompilerParams(
            collective_id=0, has_side_effects=True, vmem_limit_bytes=56 * 2**20
        ),
    )(
        query, forget, value, gate, fmin[None], eld, gain[None], wout, stream,
        ffgain.reshape(n_tp, 1, dcols), routes.T, router.T, gate_weight, up_weight, down_weight,
    )


def solution(mesh):
    both = ("sp", "tp")
    placed = (
        P("sp", "tp"), P("sp", "tp"), P("sp", "tp"), P("sp", "tp"), P("tp"), P("tp", "sp"), P("tp"),
        P(None, "tp"), P(both, None), P(), P("sp", None), P(both, None),
        P("sp", None, "tp"), P("sp", None, "tp"), P("sp", "tp", None),
    )
    return jax.shard_map(
        per_device, mesh=mesh, in_specs=placed, out_specs=P(both, None), check_vma=False
    )
```

```python
import jax
import jax.numpy as jnp
from jax import lax
from jax.experimental import pallas as pl
from jax.experimental.pallas import tpu as pltpu
from jax.sharding import PartitionSpec as P

TOPK = 2
EPSILON = 1e-06
OWNERS = 48
PLANE_ORDER = sum(offset * 8**k for k, offset in enumerate((0, 6, 2, 5, 4, 3, 7, 1)))
MESH = pl.DeviceIdType.MESH
f32 = jnp.float32
bf16 = jnp.bfloat16


def nn(a, b):
    return jnp.dot(a, b, preferred_element_type=f32)


def nt(a, b):
    return lax.dot_general(a, b, (((1,), (1,)), ((), ())), preferred_element_type=f32)


def tn(a, b):
    return lax.dot_general(a, b, (((0,), (0,)), ((), ())), preferred_element_type=f32)


def split2(x):
    hi = x.astype(bf16)
    return hi, (x - hi.astype(f32)).astype(bf16)


def split3(x):
    hi = x.astype(bf16)
    rest = x - hi.astype(f32)
    mid = rest.astype(bf16)
    return hi, mid, (rest - mid.astype(f32)).astype(bf16)


def sigmoid(x):
    return 1.0 / (1.0 + jnp.exp(-x))


def silu(x):
    return x / (1.0 + jnp.exp(-x))


def copy_to(src, dst, send, recv, target):
    return pltpu.make_async_remote_copy(
        src_ref=src, dst_ref=dst, send_sem=send, recv_sem=recv, device_id=target, device_id_type=MESH
    )


def wait_bytes(ref, sem):
    pltpu.make_async_copy(ref, ref, sem).wait()


def layer_kernel(
    q_hbm, f_hbm, v_hbm, g_hbm, fmin_ref, eld_ref, gain_ref, wout_hbm, stream_hbm, ffgain_ref,
    routes_ref, router_ref, gate_hbm, up_hbm, down_hbm,
    out_ref,
    q_ref, f_ref, v_ref, g_ref, wout, strm, msg, got, carr, back, acc, qe_hi, qe_lo, hid, ss, resid_ref,
    gate_w, up_w, down_w, relay, to_slots, from_slots, router, sendbuf, rows_in, inner, outs, returned, slices, final,
    wsem, msend, mrecv, bsend, brecv, hsend, hrecv, ssend, srecv, tsend, trecv, lsem,
    gsem, usem, dsem, dsend, drecv, psend, precv, zsend, zrecv, xsend, xrecv, isend, irecv,
    rsend, rrecv, fsend, frecv, insem,
):
    rows = q_ref.shape[0]
    half = rows // 2
    heads = q_ref.shape[1] // 128
    me = lax.axis_index("sp")
    t = lax.axis_index("tp")
    n_sp = lax.axis_size("sp")
    n_tp = lax.axis_size("tp")
    right, left = lax.rem(t + 1, n_tp), lax.rem(t + n_tp - 1, n_tp)
    opposite = lax.rem(t + 2, n_tp)
    dcols = resid_ref.shape[1]
    quarter = rows // n_tp
    width = q_ref.shape[1]

    barrier = pltpu.get_barrier_semaphore()

    @pl.loop(1, n_sp)
    def _(k):
        pl.semaphore_signal(barrier, inc=1, device_id={"sp": lax.rem(me + k, n_sp)}, device_id_type=MESH)

    for k in range(1, n_tp):
        pl.semaphore_signal(barrier, inc=1, device_id={"tp": lax.rem(t + k, n_tp)}, device_id_type=MESH)

    loads = [
        pltpu.make_async_copy(src, dst, insem.at[i])
        for i, (src, dst) in enumerate(((f_hbm, f_ref), (v_hbm, v_ref), (q_hbm, q_ref), (g_hbm, g_ref)))
    ]
    for c in loads:
        c.start()
    weight_copy = pltpu.make_async_copy(wout_hbm, wout, wsem)
    weight_copy.start()
    own_rows = pl.ds(pl.multiple_of(t * quarter, quarter), quarter)
    own_stream = pltpu.make_async_copy(
        stream_hbm.at[:, pl.ds(pl.multiple_of(t * dcols, dcols), dcols)], strm.at[own_rows], lsem
    )
    own_stream.start()
    gate_copy = pltpu.make_async_copy(gate_hbm.at[0], gate_w, gsem)
    up_copy = pltpu.make_async_copy(up_hbm.at[0], up_w, usem)
    gate_copy.start()
    up_copy.start()
    hidden_units = down_hbm.shape[1]
    own_units = pl.ds(pl.multiple_of(t * hidden_units, hidden_units), hidden_units)

    def down_part(k):
        return down_hbm.at[0, :, pl.ds(pl.multiple_of(k * dcols, dcols), dcols)]

    own_down = pltpu.make_async_copy(down_part(t), down_w.at[own_units], dsem)
    own_down.start()
    picked = router_ref[...] / (router_ref[0:1] + router_ref[1:2])
    router[t] = jnp.zeros((8, 128), f32)
    router[t, 0:TOPK, 0:quarter] = picked

    lower = (
        lax.broadcasted_iota(jnp.int32, (rows, rows), 0) >= lax.broadcasted_iota(jnp.int32, (rows, rows), 1)
    ).astype(bf16)
    loads[0].wait()
    weight = (1.0 - fmin_ref[0]) * sigmoid(-f_ref[...].astype(f32))
    d_hi, d_mid, d_lo = split3(jnp.log1p(-weight))
    decay = nn(lower, d_hi) + nn(lower, d_mid) + nn(lower, d_lo)
    e_hi, e_mid, e_lo = split3(eld_ref[...])
    extra = nt(lower, e_hi) + nt(lower, e_mid) + nt(lower, e_lo)

    loads[1].wait()
    row_of = lax.broadcasted_iota(jnp.int32, (8, 128), 0)
    parts = []
    for h in range(heads):
        lanes = slice(h * 128, (h + 1) * 128)
        run = decay[:, lanes] + extra[:, h : h + 1]
        w_h = weight[:, lanes]
        mid, end = run[half - 1 : half], run[rows - 1 : rows]
        v0, v1 = v_ref[0:half, lanes], v_ref[half:rows, lanes]
        k0_hi, k0_lo = split2(w_h[0:half] * jnp.exp(mid - run[0:half]))
        k1_hi, k1_lo = split2(w_h[half:rows] * jnp.exp(end - run[half:rows]))
        s0 = tn(v0, k0_hi) + tn(v0, k0_lo)
        s1 = tn(v1, k1_hi) + tn(v1, k1_lo)
        local = jnp.exp(end - mid) * s0 + s1
        t_hi, t_mid, t_lo = split3(end)
        tail = jnp.where(
            row_of == 0,
            t_hi.astype(f32),
            jnp.where(row_of == 1, t_mid.astype(f32), jnp.where(row_of == 2, t_lo.astype(f32), 0.0)),
        )
        piece = jnp.concatenate(
            [local.reshape(16, 8, 128), jnp.broadcast_to(tail[None], (16, 8, 128))], axis=1
        )
        msg[h * 16 : (h + 1) * 16] = piece.astype(bf16)
        parts.append((run, w_h, v0, v1, mid, s0))

    pl.semaphore_wait(barrier, n_sp + n_tp - 2)

    def owner_device(p):
        return (p // 3) * 4 + lax.rem(p, 3)

    is_owner = lax.rem(me, 4) < 3
    mine = (me // 4) * 3 + jnp.minimum(lax.rem(me, 4), 2)

    @pl.loop(0, OWNERS)
    def _(k):
        p = lax.rem(mine + k, OWNERS)
        target = owner_device(p)

        @pl.when(target != me)
        def _():
            copy_to(msg.at[p], got.at[me], msend, mrecv, {"sp": target}).start()

    for k in range(1, n_tp):
        other = lax.rem(t + k, n_tp)
        copy_to(
            stream_hbm.at[:, pl.ds(pl.multiple_of(other * dcols, dcols), dcols)],
            strm.at[own_rows],
            tsend.at[k - 1],
            trecv.at[k - 1],
            {"tp": other},
        ).start()
    shares = [
        copy_to(router.at[t], router.at[t], psend.at[k - 1], precv.at[k - 1], {"tp": lax.rem(t + k, n_tp)})
        for k in range(1, n_tp)
    ]
    for c in shares:
        c.start()

    slots = n_sp * 16
    unit = (
        lax.broadcasted_iota(jnp.int32, (rows, rows), 0) == lax.broadcasted_iota(jnp.int32, (rows, rows), 1)
    ).astype(bf16)
    first = lax.broadcasted_iota(jnp.int32, (rows, rows), 0)
    second = lax.broadcasted_iota(jnp.int32, (rows, rows), 1)
    same = (first >> 6) == (second >> 6)
    earlier = ((first < second) & same).astype(bf16)
    later = ((second < first) & same).astype(bf16)
    routes = routes_ref[...]
    slot = lax.broadcasted_iota(jnp.int32, (slots, rows), 0)
    token = lax.broadcasted_iota(jnp.int32, (slots, rows), 1)
    named = (routes[0:1] == (slot >> 4)) | (routes[1:2] == (slot >> 4))
    count = nn(named.astype(bf16), earlier)
    here = named & (count == (slot & 3).astype(f32)) & (((slot >> 2) & 3) == (token >> 6))
    to_slots[...] = here.astype(bf16)
    columns = nt(unit, routes.astype(f32).astype(bf16))
    slot = lax.broadcasted_iota(jnp.int32, (rows, slots), 1)
    token = lax.broadcasted_iota(jnp.int32, (rows, slots), 0)
    expert = (slot >> 4).astype(f32)
    chosen = [columns[:, j : j + 1] == expert for j in range(TOPK)]
    count = nn(later, (chosen[0] | chosen[1]).astype(bf16))
    fits = (count == (slot & 3).astype(f32)) & (((slot >> 2) & 3) == (token >> 6))
    for j in range(TOPK):
        from_slots[j] = (chosen[j] & fits).astype(bf16)

    loads[2].wait()
    causal = lax.broadcasted_iota(jnp.int32, (half, half), 0) >= lax.broadcasted_iota(
        jnp.int32, (half, half), 1
    )
    for h in range(heads):
        lanes = slice(h * 128, (h + 1) * 128)
        run, w_h, v0, v1, mid, s0 = parts[h]
        query = silu(q_ref[:, lanes].astype(f32))
        full_hi, full_lo = split2(query * jnp.exp(run))
        qe_hi[:, lanes] = full_hi
        qe_lo[:, lanes] = full_lo
        for c, values in ((0, v0), (1, v1)):
            span = slice(c * half, (c + 1) * half)
            centre = run[c * half + half // 2 - 1 : c * half + half // 2]
            a_hi, a_lo = split2(query[span] * jnp.exp(run[span] - centre))
            b_hi, b_lo = split2(w_h[span] * jnp.exp(centre - run[span]))
            scores = nt(a_hi, b_hi) + nt(a_hi, b_lo) + nt(a_lo, b_hi)
            p_hi, p_lo = split2(jnp.where(causal, scores, 0.0))
            out = nn(p_hi, values) + nn(p_lo, values)
            if c == 1:
                c_hi, c_lo = split2(query[span] * jnp.exp(run[span] - mid))
                z_hi, z_lo = split2(s0)
                out = out + nt(c_hi, z_hi) + nt(c_hi, z_lo) + nt(c_lo, z_hi)
            acc[span, lanes] = out

    @pl.when(is_owner)
    def _():
        got[me] = msg[mine]
        wait_bytes(got.at[pl.ds(0, n_sp - 1)], mrecv)

        def step(i, state):
            carr[i] = state.astype(bf16)
            block = got[i].astype(f32)
            total = block[8:9] + block[9:10] + block[10:11]
            return jnp.exp(total) * state + block[0:8]

        lax.fori_loop(0, n_sp, step, jnp.zeros((8, 128), f32), unroll=8)
        back[mine] = carr[me]

        @pl.loop(1, n_sp)
        def _(k):
            target = lax.rem(me + k, n_sp)
            copy_to(carr.at[target], back.at[mine], bsend, brecv, {"sp": target}).start()

    unit_half = hidden_units // 2
    down_sends = [
        copy_to(down_part(other), down_w.at[own_units], dsend.at[k], drecv.at[k], {"tp": other})
        for k, other in enumerate((right, left))
    ]
    down_sends[0].start()
    down_sends[1].start()
    loads[3].wait()
    gate = gain_ref[0] * silu(g_ref[...].astype(f32))

    @pl.when(is_owner)
    def _():
        wait_bytes(back.at[pl.ds(0, OWNERS - 1)], brecv)

    @pl.when(jnp.logical_not(is_owner))
    def _():
        wait_bytes(back.at[pl.ds(0, OWNERS)], brecv)

    for h in range(heads):
        lanes = slice(h * 128, (h + 1) * 128)
        state = back[h * 16 : (h + 1) * 16].astype(f32).reshape(128, 128).astype(bf16)
        out = acc[:, lanes] + nt(qe_hi[:, lanes], state) + nt(qe_lo[:, lanes], state)
        out = out * lax.rsqrt(jnp.mean(out * out, axis=1, keepdims=True) + EPSILON)
        hid[t, :, lanes] = (out * gate[:, lanes]).astype(bf16)

    top, low = pl.ds(0, half), pl.ds(half, half)
    to_right = [
        copy_to(hid.at[t, r], hid.at[t, r], hsend.at[i], hrecv.at[i], {"tp": right})
        for i, r in enumerate((top, low))
    ]
    to_left = [
        copy_to(hid.at[t, r], hid.at[t, r], hsend.at[2 + i], hrecv.at[2 + i], {"tp": left})
        for i, r in enumerate((low, top))
    ]
    to_right[0].start()
    to_left[0].start()
    to_right[1].start()
    to_left[1].start()
    weight_copy.wait()

    def partial(block):
        return nn(hid[block], wout[pl.ds(pl.multiple_of(block * width, width), width), :])

    proj = partial(t)
    to_right[0].wait_recv()
    on_right = copy_to(hid.at[left, top], hid.at[left, top], hsend.at[4], hrecv.at[4], {"tp": right})
    on_right.start()
    to_left[0].wait_recv()
    on_left = copy_to(hid.at[right, low], hid.at[right, low], hsend.at[5], hrecv.at[5], {"tp": left})
    on_left.start()
    to_right[1].wait_recv()
    proj = proj + partial(left)
    to_left[1].wait_recv()
    proj = proj + partial(right)
    own_stream.wait()
    for k in range(1, n_tp):
        other = lax.rem(t + k, n_tp)
        copy_to(
            stream_hbm.at[:, pl.ds(pl.multiple_of(other * dcols, dcols), dcols)],
            strm.at[own_rows],
            tsend.at[k - 1],
            trecv.at[k - 1],
            {"tp": other},
        ).wait()
    on_right.wait_recv()
    on_left.wait_recv()
    proj = proj + partial(opposite)
    resid = strm[...].astype(f32) + proj.astype(bf16).astype(f32)
    resid_ref[...] = resid
    r_hi, r_mid, r_lo = split3(resid * resid)
    ones = jnp.ones((8, dcols), bf16)
    ss[t] = nt(ones, r_hi) + nt(ones, r_mid) + nt(ones, r_lo)
    sums = []
    for k in range(1, n_tp):
        sums.append(
            copy_to(ss.at[t], ss.at[t], ssend.at[k - 1], srecv.at[k - 1], {"tp": lax.rem(t + k, n_tp)})
        )
        sums[-1].start()
    down_relay = [
        copy_to(
            down_hbm.at[0, pl.ds(s * unit_half, unit_half), pl.ds(pl.multiple_of(opposite * dcols, dcols), dcols)],
            relay.at[s],
            dsend.at[2 + s],
            drecv.at[2 + s],
            {"tp": other},
        )
        for s, other in ((0, right), (1, left))
    ]
    down_relay[0].start()
    down_relay[1].start()
    for c in sums:
        c.wait_recv()
    total = ss[0]
    for k in range(1, n_tp):
        total = total + ss[k]
    scale = lax.rsqrt(total / (n_tp * dcols) + EPSILON)
    i_hi, i_mid, i_lo = split3(scale)
    column = (nt(unit, i_hi) + nt(unit, i_mid) + nt(unit, i_lo))[:, 0:1]
    normed = (resid_ref[...] * column * ffgain_ref[t]).astype(bf16)
    sendbuf[...] = nn(to_slots[...], normed).astype(bf16)

    plane_size = 8
    planes = n_sp // plane_size
    z = me // plane_size
    b_me = lax.rem(me, plane_size)
    chunks = 2 * planes
    per_chunk = plane_size // 2
    span, part = per_chunk * 16, per_chunk * 8
    my_half = b_me // per_chunk

    def message(k):
        return pl.ds(pl.multiple_of(k * 16, 16), 16)

    def offset(plane):
        power = (1 + 7 * (plane % 2)) * (1 + 63 * ((plane // 2) % 2)) * (1 + 4095 * (plane // 4))
        return (PLANE_ORDER // power) % 8

    def source_plane(i):
        return lax.rem(z + planes - offset(i // 2), planes)

    def chunk(i):
        return (source_plane(i) * 2 + i % 2) * span

    def whole(i):
        return pl.ds(pl.multiple_of(chunk(i), span), span)

    def piece(i, s):
        return pl.ds(pl.multiple_of(chunk(i) + s * part, part), part)

    for i in range(planes):

        @pl.loop(1 if i == 0 else 0, plane_size)
        def _(k, i=i):
            target = lax.rem(z + offset(i), planes) * plane_size + lax.rem(b_me + k, plane_size)
            copy_to(
                sendbuf.at[message(target)],
                rows_in.at[t, message(me)],
                zsend,
                zrecv.at[2 * i + my_half],
                {"sp": target},
            ).start()

    rows_in[t, message(me)] = sendbuf[message(me)]
    down_last = [
        copy_to(
            relay.at[s],
            down_w.at[pl.ds(pl.multiple_of(source * hidden_units + s * unit_half, unit_half), unit_half)],
            dsend.at[4 + s],
            drecv.at[4 + s],
            {"tp": target},
        )
        for s, source, target in ((0, left, right), (1, right, left))
    ]
    for s in range(2):
        down_relay[s].wait_recv()
        down_last[s].start()
    gate_copy.wait()
    up_copy.wait()

    def ring_start(ref, i, send, recv):
        for s, target, n in ((0, right, 0), (1, left, 2), (1, right, 1), (0, left, 3)):
            here = ref.at[t, piece(i, s)]
            copy_to(here, here, send, recv.at[i, n], {"tp": target}).start()

    def ring_forward(ref, i, send, recv):
        for s, source, target, n in ((0, left, right, 0), (1, right, left, 2)):
            here = ref.at[source, piece(i, s)]
            wait_bytes(here, recv.at[i, n])
            copy_to(here, here, send, recv.at[i, 4 + s], {"tp": target}).start()

    def ring_end(ref, i, recv):
        wait_bytes(ref.at[left, piece(i, 1)], recv.at[i, 1])
        wait_bytes(ref.at[right, piece(i, 0)], recv.at[i, 3])
        wait_bytes(ref.at[opposite, piece(i, 0)], recv.at[i, 4])
        wait_bytes(ref.at[opposite, piece(i, 1)], recv.at[i, 5])

    @pl.loop(0, chunks + 4)
    def _(i):
        @pl.when(i < chunks)
        def _():
            local = (i // 2 == 0) & (i % 2 == my_half)

            @pl.when(local)
            def _():
                wait_bytes(rows_in.at[t, pl.ds(0, span - 16)], zrecv.at[i])

            @pl.when(jnp.logical_not(local))
            def _():
                wait_bytes(rows_in.at[t, whole(i)], zrecv.at[i])

            ring_start(rows_in, i, xsend, xrecv)

        @pl.when((i >= 1) & (i < chunks + 1))
        def _():
            ring_forward(rows_in, i - 1, xsend, xrecv)

        @pl.when((i >= 2) & (i < chunks + 2))
        def _():
            j = i - 2
            ring_end(rows_in, j, xrecv)
            gate_act = jnp.zeros((span, gate_w.shape[1]), f32)
            up_act = jnp.zeros((span, gate_w.shape[1]), f32)
            for k in range(n_tp):
                block = rows_in[k, whole(j)]
                gate_act = gate_act + nn(block, gate_w[k * dcols : (k + 1) * dcols])
                up_act = up_act + nn(block, up_w[k * dcols : (k + 1) * dcols])
            inner[t, whole(j)] = (silu(gate_act) * up_act).astype(bf16)
            ring_start(inner, j, isend, irecv)

        @pl.when((i >= 3) & (i < chunks + 3))
        def _():
            ring_forward(inner, i - 3, isend, irecv)

        @pl.when(i >= 4)
        def _():
            j = i - 4

            @pl.when(j == 0)
            def _():
                own_down.wait()
                for c in down_sends + down_last:
                    c.wait_recv()

            ring_end(inner, j, irecv)
            out = jnp.zeros((span, dcols), f32)
            for k in range(n_tp):
                out = out + nn(
                    inner[k, whole(j)], down_w[k * hidden_units : (k + 1) * hidden_units]
                )
            outs[whole(j)] = out.astype(bf16)

            @pl.loop(0, per_chunk)
            def _(k):
                target = (
                    source_plane(j) * plane_size + (j % 2) * per_chunk + lax.rem(b_me + k, per_chunk)
                )

                @pl.when(target != me)
                def _():
                    copy_to(
                        outs.at[message(target)], returned.at[message(me)], rsend, rrecv, {"sp": target}
                    ).start()

    returned[message(me)] = outs[message(me)]
    for c in shares:
        c.wait_recv()
    eye = (
        lax.broadcasted_iota(jnp.int32, (quarter, 128), 0) == lax.broadcasted_iota(jnp.int32, (quarter, 128), 1)
    ).astype(bf16)
    shares_of = []
    for k in range(n_tp):
        p_hi, p_mid, p_lo = split3(router[k])
        shares_of.append(nt(eye, p_hi) + nt(eye, p_mid) + nt(eye, p_lo))
    share = jnp.concatenate(shares_of, axis=0)
    wait_bytes(returned.at[pl.ds(0, slots - 16)], rrecv)
    total = resid_ref[...]
    for j in range(TOPK):
        total = total + share[:, j : j + 1] * nn(from_slots[j], returned[...])
    slices[...] = total.astype(bf16)
    own_cols = pl.ds(pl.multiple_of(t * dcols, dcols), dcols)
    last = []
    for k in range(1, n_tp):
        other = lax.rem(t + k, n_tp)
        last.append(
            copy_to(
                slices.at[pl.ds(pl.multiple_of(other * quarter, quarter), quarter)],
                final.at[:, own_cols],
                fsend.at[k - 1],
                frecv.at[k - 1],
                {"tp": other},
            )
        )
        last[-1].start()
    final[:, own_cols] = slices[own_rows]
    for c in last:
        c.wait_recv()
    out_ref[...] = final[...]
    for c in last + shares + down_sends + down_relay + down_last:
        c.wait_send()
    wait_bytes(sendbuf.at[pl.ds(0, slots - 16)], zsend)
    wait_bytes(outs.at[pl.ds(0, slots - 16)], rsend)
    wait_bytes(rows_in.at[pl.ds(0, 3)], xsend)
    wait_bytes(inner.at[pl.ds(0, 3)], isend)
    for c in sums + to_right + to_left + [on_right, on_left]:
        c.wait_send()

    @pl.when(is_owner)
    def _():
        wait_bytes(msg.at[pl.ds(0, OWNERS - 1)], msend)
        wait_bytes(carr.at[pl.ds(0, n_sp - 1)], bsend)

    @pl.when(jnp.logical_not(is_owner))
    def _():
        wait_bytes(msg.at[pl.ds(0, OWNERS)], msend)


def per_device(
    query, forget, value, gate, fmin, eld, gain, wout, stream, ffgain, routes, router,
    gate_weight, up_weight, down_weight,
):
    rows, width = query.shape
    n_sp, n_tp = lax.axis_size("sp"), lax.axis_size("tp")
    model = stream.shape[1]
    dcols = model // n_tp
    slots = n_sp * 16
    units = down_weight.shape[1]
    vmem = pl.BlockSpec(memory_space=pltpu.VMEM)
    hbm = pl.BlockSpec(memory_space=pl.ANY)
    dma = pltpu.SemaphoreType.DMA
    return pl.pallas_call(
        layer_kernel,
        name="layer",
        out_shape=jax.ShapeDtypeStruct(stream.shape, bf16),
        in_specs=[hbm] * 4 + [vmem] * 3 + [hbm, hbm] + [vmem] * 3 + [hbm] * 3,
        out_specs=vmem,
        scratch_shapes=[
            pltpu.VMEM((rows, width), bf16),
            pltpu.VMEM((rows, width), bf16),
            pltpu.VMEM((rows, width), bf16),
            pltpu.VMEM((rows, width), bf16),
            pltpu.VMEM(wout.shape, bf16),
            pltpu.VMEM((rows, dcols), bf16),
            pltpu.VMEM((OWNERS, 16, 128), bf16),
            pltpu.VMEM((n_sp, 16, 128), bf16),
            pltpu.VMEM((n_sp, 8, 128), bf16),
            pltpu.VMEM((OWNERS, 8, 128), bf16),
            pltpu.VMEM((rows, width), f32),
            pltpu.VMEM((rows, width), bf16),
            pltpu.VMEM((rows, width), bf16),
            pltpu.VMEM((n_tp, rows, width), bf16),
            pltpu.VMEM((n_tp, 8, rows), f32),
            pltpu.VMEM((rows, dcols), f32),
            pltpu.VMEM((model, units), bf16),
            pltpu.VMEM((model, units), bf16),
            pltpu.VMEM((n_tp * units, dcols), bf16),
            pltpu.VMEM((2, units // 2, dcols), bf16),
            pltpu.VMEM((slots, rows), bf16),
            pltpu.VMEM((TOPK, rows, slots), bf16),
            pltpu.VMEM((n_tp, 8, 128), f32),
            pltpu.VMEM((slots, dcols), bf16),
            pltpu.VMEM((n_tp, slots, dcols), bf16),
            pltpu.VMEM((n_tp, slots, units), bf16),
            pltpu.VMEM((slots, dcols), bf16),
            pltpu.VMEM((slots, dcols), bf16),
            pltpu.VMEM((rows, dcols), bf16),
            pltpu.VMEM(stream.shape, bf16),
            dma, dma, dma, dma, dma, dma((6,)), dma((6,)), dma((3,)), dma((3,)), dma((3,)), dma((3,)), dma,
            dma, dma, dma, dma((6,)), dma((6,)), dma((3,)), dma((3,)),
            dma, dma((16,)), dma, dma((16, 6)), dma, dma((16, 6)), dma, dma, dma((3,)), dma((3,)), dma((4,)),
        ],
        compiler_params=pltpu.CompilerParams(
            collective_id=0, has_side_effects=True, vmem_limit_bytes=56 * 2**20
        ),
    )(
        query, forget, value, gate, fmin.reshape(1, 1, width), eld, gain.reshape(1, 1, width), wout, stream,
        ffgain.reshape(n_tp, 1, dcols), routes.T, router.T, gate_weight, up_weight, down_weight,
    )


def solution(mesh):
    both = ("sp", "tp")
    placed = (
        P("sp", "tp"), P("sp", "tp"), P("sp", "tp"), P("sp", "tp"), P("tp"), P("tp", "sp"), P("tp"),
        P(None, "tp"), P(both, None), P(), P("sp", None), P(both, None),
        P("sp", None, "tp"), P("sp", None, "tp"), P("sp", "tp", None),
    )
    return jax.shard_map(
        per_device, mesh=mesh, in_specs=placed, out_specs=P(both, None), check_vma=False
    )
```

```python
import jax
import jax.numpy as jnp
from jax import lax
from jax.experimental import pallas as pl
from jax.experimental.pallas import tpu as pltpu
from jax.sharding import PartitionSpec as P

TOPK = 2
EPSILON = 1e-06
OWNERS = 48
LIMIT = 56
PLANE_ORDER = sum(offset * 8**k for k, offset in enumerate((0, 6, 2, 5, 4, 3, 7, 1)))
MESH = pl.DeviceIdType.MESH
f32 = jnp.float32
bf16 = jnp.bfloat16


def nn(a, b):
    return jnp.dot(a, b, preferred_element_type=f32)


def nt(a, b):
    return lax.dot_general(a, b, (((1,), (1,)), ((), ())), preferred_element_type=f32)


def tn(a, b):
    return lax.dot_general(a, b, (((0,), (0,)), ((), ())), preferred_element_type=f32)


def split2(x):
    hi = x.astype(bf16)
    return hi, (x - hi.astype(f32)).astype(bf16)


def split3(x):
    hi = x.astype(bf16)
    rest = x - hi.astype(f32)
    mid = rest.astype(bf16)
    return hi, mid, (rest - mid.astype(f32)).astype(bf16)


def sigmoid(x):
    return 1.0 / (1.0 + jnp.exp(-x))


def silu(x):
    return x / (1.0 + jnp.exp(-x))


def copy_to(src, dst, send, recv, target):
    return pltpu.make_async_remote_copy(
        src_ref=src, dst_ref=dst, send_sem=send, recv_sem=recv, device_id=target, device_id_type=MESH
    )


def wait_bytes(ref, sem):
    pltpu.make_async_copy(ref, ref, sem).wait()


def layer_kernel(
    q_hbm, f_hbm, v_hbm, g_hbm, fmin_ref, eld_ref, gain_ref, wout_hbm, stream_hbm, ffgain_ref,
    routes_ref, router_ref, gate_hbm, up_hbm, down_hbm,
    out_ref,
    q_ref, f_ref, v_ref, g_ref, wout, strm, msg, got, carr, back, acc, qe_hi, qe_lo, hid, resid_ref,
    gate_w, up_w, down_w, relay, to_slots, from_slots, router, sendbuf, rows_in, inner, outs, returned, slices, final,
    wsem, msend, mrecv, bsend, brecv, hsend, hrecv, tsend, trecv, lsem,
    gsem, usem, dsem, dsend, drecv, psend, precv, zsend, zrecv, xsend, xrecv, isend, irecv,
    rsend, rrecv, fsend, frecv, insem,
):
    rows = q_ref.shape[0]
    half = rows // 2
    heads = q_ref.shape[1] // 128
    me = lax.axis_index("sp")
    t = lax.axis_index("tp")
    n_sp = lax.axis_size("sp")
    n_tp = lax.axis_size("tp")
    right, left = lax.rem(t + 1, n_tp), lax.rem(t + n_tp - 1, n_tp)
    opposite = lax.rem(t + 2, n_tp)
    dcols = resid_ref.shape[1]
    quarter = rows // n_tp
    width = q_ref.shape[1]

    loads = [
        pltpu.make_async_copy(src, dst, insem.at[i])
        for i, (src, dst) in enumerate(((f_hbm, f_ref), (v_hbm, v_ref), (q_hbm, q_ref), (g_hbm, g_ref)))
    ]
    for c in loads:
        c.start()

    barrier = pltpu.get_barrier_semaphore()

    @pl.loop(1, n_sp)
    def _(k):
        pl.semaphore_signal(barrier, inc=1, device_id={"sp": lax.rem(me + k, n_sp)}, device_id_type=MESH)

    for k in range(1, n_tp):
        pl.semaphore_signal(barrier, inc=1, device_id={"tp": lax.rem(t + k, n_tp)}, device_id_type=MESH)

    weight_copy = pltpu.make_async_copy(wout_hbm, wout, wsem)
    weight_copy.start()
    own_rows = pl.ds(pl.multiple_of(t * quarter, quarter), quarter)
    own_stream = pltpu.make_async_copy(
        stream_hbm.at[:, pl.ds(pl.multiple_of(t * dcols, dcols), dcols)], strm.at[own_rows], lsem
    )
    own_stream.start()
    gate_copy = pltpu.make_async_copy(gate_hbm.at[0], gate_w, gsem)
    up_copy = pltpu.make_async_copy(up_hbm.at[0], up_w, usem)
    gate_copy.start()
    up_copy.start()
    hidden_units = down_hbm.shape[1]
    own_units = pl.ds(pl.multiple_of(t * hidden_units, hidden_units), hidden_units)

    def down_part(k):
        return down_hbm.at[0, :, pl.ds(pl.multiple_of(k * dcols, dcols), dcols)]

    own_down = pltpu.make_async_copy(down_part(t), down_w.at[own_units], dsem)
    own_down.start()
    picked = router_ref[...] / (router_ref[0:1] + router_ref[1:2])
    router[t] = jnp.zeros((8, 128), f32)
    router[t, 0:TOPK, 0:quarter] = picked

    lower = (
        lax.broadcasted_iota(jnp.int32, (rows, rows), 0) >= lax.broadcasted_iota(jnp.int32, (rows, rows), 1)
    ).astype(bf16)
    loads[0].wait()
    weight = (1.0 - fmin_ref[...].reshape(1, width)) * sigmoid(-f_ref[...].astype(f32))
    d_hi, d_mid, d_lo = split3(jnp.log1p(-weight))
    decay = nn(lower, d_hi) + nn(lower, d_mid) + nn(lower, d_lo)
    e_hi, e_mid, e_lo = split3(eld_ref[...])
    extra = nt(lower, e_hi) + nt(lower, e_mid) + nt(lower, e_lo)

    loads[1].wait()
    row_of = lax.broadcasted_iota(jnp.int32, (8, 128), 0)
    parts = []
    for h in range(heads):
        lanes = slice(h * 128, (h + 1) * 128)
        run = decay[:, lanes] + extra[:, h : h + 1]
        w_h = weight[:, lanes]
        mid, end = run[half - 1 : half], run[rows - 1 : rows]
        v0, v1 = v_ref[0:half, lanes], v_ref[half:rows, lanes]
        k0_hi, k0_lo = split2(w_h[0:half] * jnp.exp(mid - run[0:half]))
        k1_hi, k1_lo = split2(w_h[half:rows] * jnp.exp(end - run[half:rows]))
        s0 = tn(v0, k0_hi) + tn(v0, k0_lo)
        s1 = tn(v1, k1_hi) + tn(v1, k1_lo)
        local = jnp.exp(end - mid) * s0 + s1
        t_hi, t_mid, t_lo = split3(end)
        tail = jnp.where(
            row_of == 0,
            t_hi.astype(f32),
            jnp.where(row_of == 1, t_mid.astype(f32), jnp.where(row_of == 2, t_lo.astype(f32), 0.0)),
        )
        piece = jnp.concatenate(
            [local.reshape(16, 8, 128), jnp.broadcast_to(tail[None], (16, 8, 128))], axis=1
        )
        msg[h * 16 : (h + 1) * 16] = piece.astype(bf16)
        parts.append((run, w_h, v0, v1, mid, s0))

    pl.semaphore_wait(barrier, n_sp + n_tp - 2)

    def owner_device(p):
        return (p // 3) * 4 + lax.rem(p, 3)

    is_owner = lax.rem(me, 4) < 3
    mine = (me // 4) * 3 + jnp.minimum(lax.rem(me, 4), 2)

    plane_size = 8
    planes = n_sp // plane_size
    per_plane = OWNERS // planes
    z = me // plane_size
    b_me = lax.rem(me, plane_size)
    far_first = (4, 3, 5, 2, 6, 1, 7, 0)
    for away in far_first:

        @pl.loop(0, per_plane)
        def _(k, away=away):
            p = lax.rem(z + away, planes) * per_plane + lax.rem(b_me + k, per_plane)
            target = owner_device(p)

            @pl.when(target != me)
            def _():
                copy_to(msg.at[p], got.at[me], msend, mrecv, {"sp": target}).start()

    for k in range(1, n_tp):
        other = lax.rem(t + k, n_tp)
        copy_to(
            stream_hbm.at[:, pl.ds(pl.multiple_of(other * dcols, dcols), dcols)],
            strm.at[own_rows],
            tsend.at[k - 1],
            trecv.at[k - 1],
            {"tp": other},
        ).start()
    shares = [
        copy_to(router.at[t], router.at[t], psend.at[k - 1], precv.at[k - 1], {"tp": lax.rem(t + k, n_tp)})
        for k in range(1, n_tp)
    ]
    for c in shares:
        c.start()

    slots = n_sp * 16
    unit = (
        lax.broadcasted_iota(jnp.int32, (rows, rows), 0) == lax.broadcasted_iota(jnp.int32, (rows, rows), 1)
    ).astype(bf16)
    first = lax.broadcasted_iota(jnp.int32, (rows, rows), 0)
    second = lax.broadcasted_iota(jnp.int32, (rows, rows), 1)
    same = (first >> 6) == (second >> 6)
    earlier = ((first < second) & same).astype(bf16)
    later = ((second < first) & same).astype(bf16)
    routes = routes_ref[...]
    slot = lax.broadcasted_iota(jnp.int32, (slots, rows), 0)
    token = lax.broadcasted_iota(jnp.int32, (slots, rows), 1)
    named = (routes[0:1] == (slot >> 4)) | (routes[1:2] == (slot >> 4))
    count = nn(named.astype(bf16), earlier)
    here = named & (count == (slot & 3).astype(f32)) & (((slot >> 2) & 3) == (token >> 6))
    to_slots[...] = here.astype(bf16)
    columns = nt(unit, routes.astype(f32).astype(bf16))
    slot = lax.broadcasted_iota(jnp.int32, (rows, slots), 1)
    token = lax.broadcasted_iota(jnp.int32, (rows, slots), 0)
    expert = (slot >> 4).astype(f32)
    chosen = [columns[:, j : j + 1] == expert for j in range(TOPK)]
    count = nn(later, (chosen[0] | chosen[1]).astype(bf16))
    fits = (count == (slot & 3).astype(f32)) & (((slot >> 2) & 3) == (token >> 6))
    for j in range(TOPK):
        from_slots[j] = (chosen[j] & fits).astype(bf16)

    loads[2].wait()
    causal = lax.broadcasted_iota(jnp.int32, (half, half), 0) >= lax.broadcasted_iota(
        jnp.int32, (half, half), 1
    )
    for h in range(heads):
        lanes = slice(h * 128, (h + 1) * 128)
        run, w_h, v0, v1, mid, s0 = parts[h]
        query = silu(q_ref[:, lanes].astype(f32))
        full_hi, full_lo = split2(query * jnp.exp(run))
        qe_hi[:, lanes] = full_hi
        qe_lo[:, lanes] = full_lo
        for c, values in ((0, v0), (1, v1)):
            span = slice(c * half, (c + 1) * half)
            centre = run[c * half + half // 2 - 1 : c * half + half // 2]
            a_hi, a_lo = split2(query[span] * jnp.exp(run[span] - centre))
            b_hi, b_lo = split2(w_h[span] * jnp.exp(centre - run[span]))
            scores = nt(a_hi, b_hi) + nt(a_hi, b_lo) + nt(a_lo, b_hi)
            p_hi, p_lo = split2(jnp.where(causal, scores, 0.0))
            out = nn(p_hi, values) + nn(p_lo, values)
            if c == 1:
                c_hi, c_lo = split2(query[span] * jnp.exp(run[span] - mid))
                z_hi, z_lo = split2(s0)
                out = out + nt(c_hi, z_hi) + nt(c_hi, z_lo) + nt(c_lo, z_hi)
            acc[span, lanes] = out

    @pl.when(is_owner)
    def _():
        got[me] = msg[mine]
        wait_bytes(got.at[pl.ds(0, n_sp - 1)], mrecv)

        def step(i, state):
            carr[i] = state.astype(bf16)
            block = got[i].astype(f32)
            total = block[8:9] + block[9:10] + block[10:11]
            return jnp.exp(total) * state + block[0:8]

        lax.fori_loop(0, n_sp, step, jnp.zeros((8, 128), f32), unroll=8)
        back[mine] = carr[me]

        for away in far_first:

            @pl.loop(0 if away else 1, plane_size)
            def _(k, away=away):
                target = lax.rem(z + away, planes) * plane_size + lax.rem(b_me + k, plane_size)
                copy_to(carr.at[target], back.at[mine], bsend, brecv, {"sp": target}).start()

    unit_half = hidden_units // 2
    down_sends = [
        copy_to(down_part(other), down_w.at[own_units], dsend.at[k], drecv.at[k], {"tp": other})
        for k, other in enumerate((right, left))
    ]
    down_sends[0].start()
    down_sends[1].start()
    loads[3].wait()
    gate = gain_ref[...].reshape(1, width) * silu(g_ref[...].astype(f32))

    @pl.when(is_owner)
    def _():
        wait_bytes(back.at[pl.ds(0, OWNERS - 1)], brecv)

    @pl.when(jnp.logical_not(is_owner))
    def _():
        wait_bytes(back.at[pl.ds(0, OWNERS)], brecv)

    for h in range(heads):
        lanes = slice(h * 128, (h + 1) * 128)
        state = back[h * 16 : (h + 1) * 16].astype(f32).reshape(128, 128).astype(bf16)
        out = acc[:, lanes] + nt(qe_hi[:, lanes], state) + nt(qe_lo[:, lanes], state)
        out = out * lax.rsqrt(jnp.mean(out * out, axis=1, keepdims=True) + EPSILON)
        hid[t, :, lanes] = (out * gate[:, lanes]).astype(bf16)

    top, low = pl.ds(0, half), pl.ds(half, half)
    to_right = [
        copy_to(hid.at[t, r], hid.at[t, r], hsend.at[i], hrecv.at[i], {"tp": right})
        for i, r in enumerate((top, low))
    ]
    to_left = [
        copy_to(hid.at[t, r], hid.at[t, r], hsend.at[2 + i], hrecv.at[2 + i], {"tp": left})
        for i, r in enumerate((low, top))
    ]
    to_right[0].start()
    to_left[0].start()
    to_right[1].start()
    to_left[1].start()
    weight_copy.wait()

    def partial(block):
        return nn(hid[block], wout[pl.ds(pl.multiple_of(block * width, width), width), :])

    proj = partial(t)
    to_right[0].wait_recv()
    on_right = copy_to(hid.at[left, top], hid.at[left, top], hsend.at[4], hrecv.at[4], {"tp": right})
    on_right.start()
    to_left[0].wait_recv()
    on_left = copy_to(hid.at[right, low], hid.at[right, low], hsend.at[5], hrecv.at[5], {"tp": left})
    on_left.start()
    to_right[1].wait_recv()
    proj = proj + partial(left)
    to_left[1].wait_recv()
    proj = proj + partial(right)
    own_stream.wait()
    for k in range(1, n_tp):
        other = lax.rem(t + k, n_tp)
        copy_to(
            stream_hbm.at[:, pl.ds(pl.multiple_of(other * dcols, dcols), dcols)],
            strm.at[own_rows],
            tsend.at[k - 1],
            trecv.at[k - 1],
            {"tp": other},
        ).wait()
    on_right.wait_recv()
    on_left.wait_recv()
    proj = proj + partial(opposite)
    down_relay = [
        copy_to(
            down_hbm.at[0, pl.ds(s * unit_half, unit_half), pl.ds(pl.multiple_of(opposite * dcols, dcols), dcols)],
            relay.at[s],
            dsend.at[2 + s],
            drecv.at[2 + s],
            {"tp": other},
        )
        for s, other in ((0, right), (1, left))
    ]
    down_relay[0].start()
    down_relay[1].start()
    resid = strm[...].astype(f32) + proj.astype(bf16).astype(f32)
    resid_ref[...] = resid
    rounded = resid.astype(bf16)

    chunks = 2 * planes
    per_chunk = plane_size // 2
    span, part = per_chunk * 16, per_chunk * 8
    my_half = b_me // per_chunk

    def message(k):
        return pl.ds(pl.multiple_of(k * 16, 16), 16)

    def offset(plane):
        power = (1 + 7 * (plane % 2)) * (1 + 63 * ((plane // 2) % 2)) * (1 + 4095 * (plane // 4))
        return (PLANE_ORDER // power) % 8

    def source_plane(i):
        return lax.rem(z + planes - offset(i // 2), planes)

    def chunk(i):
        return (source_plane(i) * 2 + i % 2) * span

    def whole(i):
        return pl.ds(pl.multiple_of(chunk(i), span), span)

    def piece(i, s):
        return pl.ds(pl.multiple_of(chunk(i) + s * part, part), part)

    for i in range(planes):
        there = lax.rem(z + offset(i), planes)
        block = pl.ds(pl.multiple_of(there * 2 * span, 2 * span), 2 * span)
        sendbuf[block] = nn(to_slots[block], rounded).astype(bf16)

        @pl.loop(1 if i == 0 else 0, plane_size)
        def _(k, i=i, there=there):
            target = there * plane_size + lax.rem(b_me + k, plane_size)
            copy_to(
                sendbuf.at[message(target)],
                rows_in.at[t, message(me)],
                zsend,
                zrecv.at[2 * i + my_half],
                {"sp": target},
            ).start()

    rows_in[t, message(me)] = sendbuf[message(me)]
    down_last = [
        copy_to(
            relay.at[s],
            down_w.at[pl.ds(pl.multiple_of(source * hidden_units + s * unit_half, unit_half), unit_half)],
            dsend.at[4 + s],
            drecv.at[4 + s],
            {"tp": target},
        )
        for s, source, target in ((0, left, right), (1, right, left))
    ]
    for s in range(2):
        down_relay[s].wait_recv()
        down_last[s].start()
    gate_copy.wait()
    up_copy.wait()

    early = chunks - 4

    def ring_start(ref, i, send, recv):
        for s, target, n in ((0, right, 0), (1, left, 2), (1, right, 1), (0, left, 3)):
            here = ref.at[t, piece(i, s)]
            copy_to(here, here, send, recv.at[i, n], {"tp": target}).start()

    def ring_forward(ref, i, send, recv):
        for s, source, target, n in ((0, left, right, 0), (1, right, left, 2)):
            here = ref.at[source, piece(i, s)]
            wait_bytes(here, recv.at[i, n])
            copy_to(here, here, send, recv.at[i, 4 + s], {"tp": target}).start()

    def ring_end(ref, i, recv):
        wait_bytes(ref.at[left, piece(i, 1)], recv.at[i, 1])
        wait_bytes(ref.at[right, piece(i, 0)], recv.at[i, 3])
        wait_bytes(ref.at[opposite, piece(i, 0)], recv.at[i, 4])
        wait_bytes(ref.at[opposite, piece(i, 1)], recv.at[i, 5])

    @pl.loop(0, chunks + 4)
    def _(i):
        @pl.when(i < chunks)
        def _():
            local = (i // 2 == 0) & (i % 2 == my_half)

            @pl.when(local)
            def _():
                wait_bytes(rows_in.at[t, pl.ds(0, span - 16)], zrecv.at[i])

            @pl.when(jnp.logical_not(local))
            def _():
                wait_bytes(rows_in.at[t, whole(i)], zrecv.at[i])

            ring_start(rows_in, i, xsend, xrecv)

        @pl.when((i >= 1) & (i < chunks + 1))
        def _():
            ring_forward(rows_in, i - 1, xsend, xrecv)

        @pl.when((i >= 2) & (i < chunks + 2))
        def _():
            j = i - 2
            ring_end(rows_in, j, xrecv)
            gate_act = jnp.zeros((span, gate_w.shape[1]), f32)
            up_act = jnp.zeros((span, gate_w.shape[1]), f32)
            squares = jnp.zeros((span, 1), f32)
            for k in range(n_tp):
                values = rows_in[k, whole(j)].astype(f32)
                squares = squares + jnp.sum(values * values, axis=1, keepdims=True)
                block = (values * ffgain_ref[k]).astype(bf16)
                gate_act = gate_act + nn(block, gate_w[k * dcols : (k + 1) * dcols])
                up_act = up_act + nn(block, up_w[k * dcols : (k + 1) * dcols])
            scale = lax.rsqrt(squares / (n_tp * dcols) + EPSILON)
            gate_act = gate_act * scale
            up_act = up_act * scale
            inner[t, whole(j)] = (silu(gate_act) * up_act).astype(bf16)
            ring_start(inner, j, isend, irecv)

        @pl.when((i >= 3) & (i < chunks + 3))
        def _():
            ring_forward(inner, i - 3, isend, irecv)

        @pl.when(i >= 4)
        def _():
            j = i - 4

            @pl.when(j == 0)
            def _():
                own_down.wait()
                for c in down_sends + down_last:
                    c.wait_recv()

            ring_end(inner, j, irecv)
            out = jnp.zeros((span, dcols), f32)
            for k in range(n_tp):
                out = out + nn(
                    inner[k, whole(j)], down_w[k * hidden_units : (k + 1) * hidden_units]
                )
            outs[whole(j)] = out.astype(bf16)

            @pl.loop(0, per_chunk)
            def _(k):
                target = (
                    source_plane(j) * plane_size + (j % 2) * per_chunk + lax.rem(b_me + k, per_chunk)
                )

                @pl.when(target != me)
                def _():
                    copy_to(
                        outs.at[message(target)],
                        returned.at[message(me)],
                        rsend,
                        rrecv.at[j // early],
                        {"sp": target},
                    ).start()

    returned[message(me)] = outs[message(me)]
    for c in shares:
        c.wait_recv()
    eye = (
        lax.broadcasted_iota(jnp.int32, (quarter, 128), 0) == lax.broadcasted_iota(jnp.int32, (quarter, 128), 1)
    ).astype(bf16)
    shares_of = []
    for k in range(n_tp):
        p_hi, p_mid, p_lo = split3(router[k])
        shares_of.append(nt(eye, p_hi) + nt(eye, p_mid) + nt(eye, p_lo))
    share = jnp.concatenate(shares_of, axis=0)
    total = resid_ref[...]
    wait_bytes(returned.at[pl.ds(0, early * span - 16)], rrecv.at[0])
    for i in range(planes):
        if i == early // 2:
            wait_bytes(returned.at[pl.ds(0, (chunks - early) * span)], rrecv.at[1])
        there = lax.rem(z + offset(i), planes)
        block = pl.ds(pl.multiple_of(there * 2 * span, 2 * span), 2 * span)
        values = returned[block]
        for j in range(TOPK):
            total = total + share[:, j : j + 1] * nn(from_slots[j, :, block], values)
    slices[...] = total.astype(bf16)
    own_cols = pl.ds(pl.multiple_of(t * dcols, dcols), dcols)
    last = []
    for k in range(1, n_tp):
        other = lax.rem(t + k, n_tp)
        last.append(
            copy_to(
                slices.at[pl.ds(pl.multiple_of(other * quarter, quarter), quarter)],
                final.at[:, own_cols],
                fsend.at[k - 1],
                frecv.at[k - 1],
                {"tp": other},
            )
        )
        last[-1].start()
    final[:, own_cols] = slices[own_rows]
    for c in last:
        c.wait_recv()
    out_ref[...] = final[...]
    for c in last + shares + down_sends + down_relay + down_last:
        c.wait_send()
    wait_bytes(sendbuf.at[pl.ds(0, slots - 16)], zsend)
    wait_bytes(outs.at[pl.ds(0, slots - 16)], rsend)
    wait_bytes(rows_in.at[pl.ds(0, 3)], xsend)
    wait_bytes(inner.at[pl.ds(0, 3)], isend)
    for c in to_right + to_left + [on_right, on_left]:
        c.wait_send()

    @pl.when(is_owner)
    def _():
        wait_bytes(msg.at[pl.ds(0, OWNERS - 1)], msend)
        wait_bytes(carr.at[pl.ds(0, n_sp - 1)], bsend)

    @pl.when(jnp.logical_not(is_owner))
    def _():
        wait_bytes(msg.at[pl.ds(0, OWNERS)], msend)


def per_device(
    query, forget, value, gate, fmin, eld, gain, wout, stream, ffgain, routes, router,
    gate_weight, up_weight, down_weight,
):
    rows, width = query.shape
    n_sp, n_tp = lax.axis_size("sp"), lax.axis_size("tp")
    model = stream.shape[1]
    dcols = model // n_tp
    slots = n_sp * 16
    units = down_weight.shape[1]
    vmem = pl.BlockSpec(memory_space=pltpu.VMEM)
    hbm = pl.BlockSpec(memory_space=pl.ANY)
    dma = pltpu.SemaphoreType.DMA
    return pl.pallas_call(
        layer_kernel,
        name="layer",
        out_shape=jax.ShapeDtypeStruct(stream.shape, bf16),
        in_specs=[hbm] * 4 + [vmem] * 3 + [hbm, hbm] + [vmem] * 3 + [hbm] * 3,
        out_specs=vmem,
        scratch_shapes=[
            pltpu.VMEM((rows, width), bf16),
            pltpu.VMEM((rows, width), bf16),
            pltpu.VMEM((rows, width), bf16),
            pltpu.VMEM((rows, width), bf16),
            pltpu.VMEM(wout.shape, bf16),
            pltpu.VMEM((rows, dcols), bf16),
            pltpu.VMEM((OWNERS, 16, 128), bf16),
            pltpu.VMEM((n_sp, 16, 128), bf16),
            pltpu.VMEM((n_sp, 8, 128), bf16),
            pltpu.VMEM((OWNERS, 8, 128), bf16),
            pltpu.VMEM((rows, width), f32),
            pltpu.VMEM((rows, width), bf16),
            pltpu.VMEM((rows, width), bf16),
            pltpu.VMEM((n_tp, rows, width), bf16),
            pltpu.VMEM((rows, dcols), f32),
            pltpu.VMEM((model, units), bf16),
            pltpu.VMEM((model, units), bf16),
            pltpu.VMEM((n_tp * units, dcols), bf16),
            pltpu.VMEM((2, units // 2, dcols), bf16),
            pltpu.VMEM((slots, rows), bf16),
            pltpu.VMEM((TOPK, rows, slots), bf16),
            pltpu.VMEM((n_tp, 8, 128), f32),
            pltpu.VMEM((slots, dcols), bf16),
            pltpu.VMEM((n_tp, slots, dcols), bf16),
            pltpu.VMEM((n_tp, slots, units), bf16),
            pltpu.VMEM((slots, dcols), bf16),
            pltpu.VMEM((slots, dcols), bf16),
            pltpu.VMEM((rows, dcols), bf16),
            pltpu.VMEM(stream.shape, bf16),
            dma, dma, dma, dma, dma, dma((6,)), dma((6,)), dma((3,)), dma((3,)), dma,
            dma, dma, dma, dma((6,)), dma((6,)), dma((3,)), dma((3,)),
            dma, dma((16,)), dma, dma((16, 6)), dma, dma((16, 6)), dma, dma((2,)), dma((3,)), dma((3,)), dma((4,)),
        ],
        compiler_params=pltpu.CompilerParams(
            collective_id=0, has_side_effects=True, vmem_limit_bytes=LIMIT * 2**20
        ),
    )(
        query, forget, value, gate, fmin, eld, gain, wout, stream,
        ffgain.reshape(n_tp, 1, dcols), routes.T, router.T, gate_weight, up_weight, down_weight,
    )


def solution(mesh):
    both = ("sp", "tp")
    placed = (
        P("sp", "tp"), P("sp", "tp"), P("sp", "tp"), P("sp", "tp"), P("tp"), P("tp", "sp"), P("tp"),
        P(None, "tp"), P(both, None), P(), P("sp", None), P(both, None),
        P("sp", None, "tp"), P("sp", None, "tp"), P("sp", "tp", None),
    )
    return jax.shard_map(
        per_device, mesh=mesh, in_specs=placed, out_specs=P(both, None), check_vma=False
    )
```

```python
import jax
import jax.numpy as jnp
from jax import lax
from jax.experimental import pallas as pl
from jax.experimental.pallas import tpu as pltpu
from jax.sharding import PartitionSpec as P

TOPK = 2
EPSILON = 1e-06
OWNERS = 48
LIMIT = 56
PLANE_ORDER = sum(offset * 8**k for k, offset in enumerate((0, 6, 2, 5, 4, 3, 7, 1)))
MESH = pl.DeviceIdType.MESH
f32 = jnp.float32
bf16 = jnp.bfloat16


def nn(a, b):
    return jnp.dot(a, b, preferred_element_type=f32)


def nt(a, b):
    return lax.dot_general(a, b, (((1,), (1,)), ((), ())), preferred_element_type=f32)


def tn(a, b):
    return lax.dot_general(a, b, (((0,), (0,)), ((), ())), preferred_element_type=f32)


def split2(x):
    hi = x.astype(bf16)
    return hi, (x - hi.astype(f32)).astype(bf16)


def split3(x):
    hi = x.astype(bf16)
    rest = x - hi.astype(f32)
    mid = rest.astype(bf16)
    return hi, mid, (rest - mid.astype(f32)).astype(bf16)


def sigmoid(x):
    return 1.0 / (1.0 + jnp.exp(-x))


def silu(x):
    return x / (1.0 + jnp.exp(-x))


def copy_to(src, dst, send, recv, target):
    return pltpu.make_async_remote_copy(
        src_ref=src, dst_ref=dst, send_sem=send, recv_sem=recv, device_id=target, device_id_type=MESH
    )


def wait_bytes(ref, sem):
    pltpu.make_async_copy(ref, ref, sem).wait()


def layer_kernel(
    q_hbm, f_hbm, v_hbm, g_hbm, fmin_ref, eld_ref, gain_ref, wout_hbm, stream_hbm, ffgain_ref,
    routes_ref, router_ref, gate_hbm, up_hbm, down_hbm,
    out_ref,
    q_ref, f_ref, v_ref, g_ref, wout, strm, msg, got, carr, back, acc, qe_hi, qe_lo, hid, resid_ref,
    gate_w, up_w, down_w, relay, to_slots, from_slots, router, sendbuf, rows_in, inner, outs, returned, slices,
    wsem, msend, mrecv, bsend, brecv, hsend, hrecv, tsend, trecv, lsem,
    gsem, usem, dsem, dsend, drecv, psend, precv, zsend, zrecv, xsend, xrecv, isend, irecv,
    rsend, rrecv, fsend, frecv, insem, osem,
):
    rows = q_ref.shape[0]
    half = rows // 2
    heads = q_ref.shape[1] // 128
    me = lax.axis_index("sp")
    t = lax.axis_index("tp")
    n_sp = lax.axis_size("sp")
    n_tp = lax.axis_size("tp")
    right, left = lax.rem(t + 1, n_tp), lax.rem(t + n_tp - 1, n_tp)
    opposite = lax.rem(t + 2, n_tp)
    dcols = resid_ref.shape[1]
    quarter = rows // n_tp
    width = q_ref.shape[1]

    loads = [
        pltpu.make_async_copy(src, dst, insem.at[i])
        for i, (src, dst) in enumerate(((f_hbm, f_ref), (v_hbm, v_ref), (q_hbm, q_ref), (g_hbm, g_ref)))
    ]
    for c in loads:
        c.start()

    barrier = pltpu.get_barrier_semaphore()

    @pl.loop(1, n_sp)
    def _(k):
        pl.semaphore_signal(barrier, inc=1, device_id={"sp": lax.rem(me + k, n_sp)}, device_id_type=MESH)

    for k in range(1, n_tp):
        pl.semaphore_signal(barrier, inc=1, device_id={"tp": lax.rem(t + k, n_tp)}, device_id_type=MESH)

    weight_copy = pltpu.make_async_copy(wout_hbm, wout, wsem)
    weight_copy.start()
    own_rows = pl.ds(pl.multiple_of(t * quarter, quarter), quarter)
    own_stream = pltpu.make_async_copy(
        stream_hbm.at[:, pl.ds(pl.multiple_of(t * dcols, dcols), dcols)], strm.at[own_rows], lsem
    )
    own_stream.start()
    gate_copy = pltpu.make_async_copy(gate_hbm.at[0], gate_w, gsem)
    up_copy = pltpu.make_async_copy(up_hbm.at[0], up_w, usem)
    gate_copy.start()
    up_copy.start()
    hidden_units = down_hbm.shape[1]
    own_units = pl.ds(pl.multiple_of(t * hidden_units, hidden_units), hidden_units)

    def down_part(k):
        return down_hbm.at[0, :, pl.ds(pl.multiple_of(k * dcols, dcols), dcols)]

    own_down = pltpu.make_async_copy(down_part(t), down_w.at[own_units], dsem)
    own_down.start()
    picked = router_ref[...] / (router_ref[0:1] + router_ref[1:2])
    router[t] = jnp.zeros((8, 128), f32)
    router[t, 0:TOPK, 0:quarter] = picked

    lower = (
        lax.broadcasted_iota(jnp.int32, (rows, rows), 0) >= lax.broadcasted_iota(jnp.int32, (rows, rows), 1)
    ).astype(bf16)
    loads[0].wait()
    weight = (1.0 - fmin_ref[...].reshape(1, width)) * sigmoid(-f_ref[...].astype(f32))
    d_hi, d_mid, d_lo = split3(jnp.log1p(-weight))
    decay = nn(lower, d_hi) + nn(lower, d_mid) + nn(lower, d_lo)
    e_hi, e_mid, e_lo = split3(eld_ref[...])
    extra = nt(lower, e_hi) + nt(lower, e_mid) + nt(lower, e_lo)

    loads[1].wait()
    row_of = lax.broadcasted_iota(jnp.int32, (8, 128), 0)
    parts = []
    for h in range(heads):
        lanes = slice(h * 128, (h + 1) * 128)
        run = decay[:, lanes] + extra[:, h : h + 1]
        w_h = weight[:, lanes]
        mid, end = run[half - 1 : half], run[rows - 1 : rows]
        v0, v1 = v_ref[0:half, lanes], v_ref[half:rows, lanes]
        k0_hi, k0_lo = split2(w_h[0:half] * jnp.exp(mid - run[0:half]))
        k1_hi, k1_lo = split2(w_h[half:rows] * jnp.exp(end - run[half:rows]))
        s0 = tn(v0, k0_hi) + tn(v0, k0_lo)
        s1 = tn(v1, k1_hi) + tn(v1, k1_lo)
        local = jnp.exp(end - mid) * s0 + s1
        t_hi, t_mid, t_lo = split3(end)
        tail = jnp.where(
            row_of == 0,
            t_hi.astype(f32),
            jnp.where(row_of == 1, t_mid.astype(f32), jnp.where(row_of == 2, t_lo.astype(f32), 0.0)),
        )
        piece = jnp.concatenate(
            [local.reshape(16, 8, 128), jnp.broadcast_to(tail[None], (16, 8, 128))], axis=1
        )
        msg[h * 16 : (h + 1) * 16] = piece.astype(bf16)
        parts.append((run, w_h, v0, v1, mid, s0))

    pl.semaphore_wait(barrier, n_sp + n_tp - 2)

    def owner_device(p):
        return (p // 3) * 4 + lax.rem(p, 3)

    is_owner = lax.rem(me, 4) < 3
    mine = (me // 4) * 3 + jnp.minimum(lax.rem(me, 4), 2)

    plane_size = 8
    planes = n_sp // plane_size
    per_plane = OWNERS // planes
    z = me // plane_size
    b_me = lax.rem(me, plane_size)
    far_first = (4, 3, 5, 2, 6, 1, 7, 0)
    for away in far_first:

        @pl.loop(0, per_plane)
        def _(k, away=away):
            p = lax.rem(z + away, planes) * per_plane + lax.rem(b_me + k, per_plane)
            target = owner_device(p)

            @pl.when(target != me)
            def _():
                copy_to(msg.at[p], got.at[me], msend, mrecv, {"sp": target}).start()

    for k in range(1, n_tp):
        other = lax.rem(t + k, n_tp)
        copy_to(
            stream_hbm.at[:, pl.ds(pl.multiple_of(other * dcols, dcols), dcols)],
            strm.at[own_rows],
            tsend.at[k - 1],
            trecv.at[k - 1],
            {"tp": other},
        ).start()
    shares = [
        copy_to(router.at[t], router.at[t], psend.at[k - 1], precv.at[k - 1], {"tp": lax.rem(t + k, n_tp)})
        for k in range(1, n_tp)
    ]
    for c in shares:
        c.start()

    unit_half = hidden_units // 2
    down_sends = [
        copy_to(down_part(other), down_w.at[own_units], dsend.at[k], drecv.at[k], {"tp": other})
        for k, other in enumerate((right, left))
    ]
    down_sends[0].start()
    down_sends[1].start()
    slots = n_sp * 16
    unit = (
        lax.broadcasted_iota(jnp.int32, (rows, rows), 0) == lax.broadcasted_iota(jnp.int32, (rows, rows), 1)
    ).astype(bf16)
    first = lax.broadcasted_iota(jnp.int32, (rows, rows), 0)
    second = lax.broadcasted_iota(jnp.int32, (rows, rows), 1)
    same = (first >> 6) == (second >> 6)
    earlier = ((first < second) & same).astype(bf16)
    later = ((second < first) & same).astype(bf16)
    routes = routes_ref[...]
    slot = lax.broadcasted_iota(jnp.int32, (slots, rows), 0)
    token = lax.broadcasted_iota(jnp.int32, (slots, rows), 1)
    named = (routes[0:1] == (slot >> 4)) | (routes[1:2] == (slot >> 4))
    count = nn(named.astype(bf16), earlier)
    here = named & (count == (slot & 3).astype(f32)) & (((slot >> 2) & 3) == (token >> 6))
    to_slots[...] = here.astype(bf16)
    columns = nt(unit, routes.astype(f32).astype(bf16))
    slot = lax.broadcasted_iota(jnp.int32, (rows, slots), 1)
    token = lax.broadcasted_iota(jnp.int32, (rows, slots), 0)
    expert = (slot >> 4).astype(f32)
    chosen = [columns[:, j : j + 1] == expert for j in range(TOPK)]
    count = nn(later, (chosen[0] | chosen[1]).astype(bf16))
    fits = (count == (slot & 3).astype(f32)) & (((slot >> 2) & 3) == (token >> 6))
    for j in range(TOPK):
        from_slots[j] = (chosen[j] & fits).astype(bf16)

    loads[2].wait()
    causal = lax.broadcasted_iota(jnp.int32, (half, half), 0) >= lax.broadcasted_iota(
        jnp.int32, (half, half), 1
    )
    for h in range(heads):
        lanes = slice(h * 128, (h + 1) * 128)
        run, w_h, v0, v1, mid, s0 = parts[h]
        query = silu(q_ref[:, lanes].astype(f32))
        full_hi, full_lo = split2(query * jnp.exp(run))
        qe_hi[:, lanes] = full_hi
        qe_lo[:, lanes] = full_lo
        for c, values in ((0, v0), (1, v1)):
            span = slice(c * half, (c + 1) * half)
            centre = run[c * half + half // 2 - 1 : c * half + half // 2]
            a_hi, a_lo = split2(query[span] * jnp.exp(run[span] - centre))
            b_hi, b_lo = split2(w_h[span] * jnp.exp(centre - run[span]))
            scores = nt(a_hi, b_hi) + nt(a_hi, b_lo) + nt(a_lo, b_hi)
            p_hi, p_lo = split2(jnp.where(causal, scores, 0.0))
            out = nn(p_hi, values) + nn(p_lo, values)
            if c == 1:
                c_hi, c_lo = split2(query[span] * jnp.exp(run[span] - mid))
                z_hi, z_lo = split2(s0)
                out = out + nt(c_hi, z_hi) + nt(c_hi, z_lo) + nt(c_lo, z_hi)
            acc[span, lanes] = out

    @pl.when(is_owner)
    def _():
        got[me] = msg[mine]
        wait_bytes(got.at[pl.ds(0, n_sp - 1)], mrecv)

        def step(i, state):
            carr[i] = state.astype(bf16)
            block = got[i].astype(f32)
            total = block[8:9] + block[9:10] + block[10:11]
            return jnp.exp(total) * state + block[0:8]

        lax.fori_loop(0, n_sp, step, jnp.zeros((8, 128), f32), unroll=8)
        back[mine] = carr[me]

        for away in far_first:

            @pl.loop(0 if away else 1, plane_size)
            def _(k, away=away):
                target = lax.rem(z + away, planes) * plane_size + lax.rem(b_me + k, plane_size)
                copy_to(carr.at[target], back.at[mine], bsend, brecv, {"sp": target}).start()

    loads[3].wait()
    gate = gain_ref[...].reshape(1, width) * silu(g_ref[...].astype(f32))

    @pl.when(is_owner)
    def _():
        wait_bytes(back.at[pl.ds(0, OWNERS - 1)], brecv)

    @pl.when(jnp.logical_not(is_owner))
    def _():
        wait_bytes(back.at[pl.ds(0, OWNERS)], brecv)

    for h in range(heads):
        lanes = slice(h * 128, (h + 1) * 128)
        state = back[h * 16 : (h + 1) * 16].astype(f32).reshape(128, 128).astype(bf16)
        out = acc[:, lanes] + nt(qe_hi[:, lanes], state) + nt(qe_lo[:, lanes], state)
        out = out * lax.rsqrt(jnp.mean(out * out, axis=1, keepdims=True) + EPSILON)
        hid[t, :, lanes] = (out * gate[:, lanes]).astype(bf16)

    top, low = pl.ds(0, half), pl.ds(half, half)
    to_right = [
        copy_to(hid.at[t, r], hid.at[t, r], hsend.at[i], hrecv.at[i], {"tp": right})
        for i, r in enumerate((top, low))
    ]
    to_left = [
        copy_to(hid.at[t, r], hid.at[t, r], hsend.at[2 + i], hrecv.at[2 + i], {"tp": left})
        for i, r in enumerate((low, top))
    ]
    to_right[0].start()
    to_left[0].start()
    to_right[1].start()
    to_left[1].start()
    weight_copy.wait()

    def partial(block):
        return nn(hid[block], wout[pl.ds(pl.multiple_of(block * width, width), width), :])

    proj = partial(t)
    to_right[0].wait_recv()
    on_right = copy_to(hid.at[left, top], hid.at[left, top], hsend.at[4], hrecv.at[4], {"tp": right})
    on_right.start()
    to_left[0].wait_recv()
    on_left = copy_to(hid.at[right, low], hid.at[right, low], hsend.at[5], hrecv.at[5], {"tp": left})
    on_left.start()
    down_relay = [
        copy_to(
            down_hbm.at[0, pl.ds(s * unit_half, unit_half), pl.ds(pl.multiple_of(opposite * dcols, dcols), dcols)],
            relay.at[s],
            dsend.at[2 + s],
            drecv.at[2 + s],
            {"tp": other},
        )
        for s, other in ((0, right), (1, left))
    ]
    down_relay[0].start()
    down_relay[1].start()
    to_right[1].wait_recv()
    proj = proj + partial(left)
    to_left[1].wait_recv()
    proj = proj + partial(right)
    own_stream.wait()
    for k in range(1, n_tp):
        other = lax.rem(t + k, n_tp)
        copy_to(
            stream_hbm.at[:, pl.ds(pl.multiple_of(other * dcols, dcols), dcols)],
            strm.at[own_rows],
            tsend.at[k - 1],
            trecv.at[k - 1],
            {"tp": other},
        ).wait()
    on_right.wait_recv()
    on_left.wait_recv()
    proj = proj + partial(opposite)
    resid = strm[...].astype(f32) + proj.astype(bf16).astype(f32)
    resid_ref[...] = resid
    rounded = resid.astype(bf16)

    chunks = 2 * planes
    per_chunk = plane_size // 2
    span, part = per_chunk * 16, per_chunk * 8
    my_half = b_me // per_chunk

    def message(k):
        return pl.ds(pl.multiple_of(k * 16, 16), 16)

    def offset(plane):
        power = (1 + 7 * (plane % 2)) * (1 + 63 * ((plane // 2) % 2)) * (1 + 4095 * (plane // 4))
        return (PLANE_ORDER // power) % 8

    def plane_half(i):
        last = i // (chunks - 4)
        plane = (1 - last) * (i // 2) + last * (planes - 2 + i % 2)
        return plane, (1 - last) * (i % 2) + last * ((i // 2) % 2)

    def source_plane(i):
        return lax.rem(z + planes - offset(plane_half(i)[0]), planes)

    def chunk(i):
        return (source_plane(i) * 2 + plane_half(i)[1]) * span

    def whole(i):
        return pl.ds(pl.multiple_of(chunk(i), span), span)

    def piece(i, s):
        return pl.ds(pl.multiple_of(chunk(i) + s * part, part), part)

    for i in range(planes):
        there = lax.rem(z + offset(i), planes)
        block = pl.ds(pl.multiple_of(there * 2 * span, 2 * span), 2 * span)
        sendbuf[block] = nn(to_slots[block], rounded).astype(bf16)

        @pl.loop(1 if i == 0 else 0, plane_size)
        def _(k, i=i, there=there):
            target = there * plane_size + lax.rem(b_me + k, plane_size)
            copy_to(
                sendbuf.at[message(target)],
                rows_in.at[t, message(me)],
                zsend,
                zrecv.at[2 * i + my_half],
                {"sp": target},
            ).start()

    rows_in[t, message(me)] = sendbuf[message(me)]
    down_last = [
        copy_to(
            relay.at[s],
            down_w.at[pl.ds(pl.multiple_of(source * hidden_units + s * unit_half, unit_half), unit_half)],
            dsend.at[4 + s],
            drecv.at[4 + s],
            {"tp": target},
        )
        for s, source, target in ((0, left, right), (1, right, left))
    ]
    for s in range(2):
        down_relay[s].wait_recv()
        down_last[s].start()
    gate_copy.wait()
    up_copy.wait()

    early = chunks - 4

    def ring_start(ref, i, send, recv):
        for s, target, n in ((0, right, 0), (1, left, 0), (1, right, 1), (0, left, 1)):
            here = ref.at[t, piece(i, s)]
            copy_to(here, here, send, recv.at[i, n], {"tp": target}).start()

    def ring_forward(ref, i, send, recv):
        wait_bytes(ref.at[t, whole(i)], recv.at[i, 0])
        for s, source, target in ((0, left, right), (1, right, left)):
            here = ref.at[source, piece(i, s)]
            copy_to(here, here, send, recv.at[i, 1], {"tp": target}).start()

    def ring_end(ref, i, recv):
        wait_bytes(ref.at[t, pl.ds(0, 2 * span)], recv.at[i, 1])

    @pl.loop(0, chunks + 4)
    def _(i):
        @pl.when(i < chunks)
        def _():
            plane, half_of = plane_half(i)
            arrival = zrecv.at[2 * plane + half_of]
            local = (plane == 0) & (half_of == my_half)

            @pl.when(local)
            def _():
                wait_bytes(rows_in.at[t, pl.ds(0, span - 16)], arrival)

            @pl.when(jnp.logical_not(local))
            def _():
                wait_bytes(rows_in.at[t, whole(i)], arrival)

            ring_start(rows_in, i, xsend, xrecv)

        @pl.when((i >= 1) & (i < chunks + 1))
        def _():
            ring_forward(rows_in, i - 1, xsend, xrecv)

        @pl.when((i >= 2) & (i < chunks + 2))
        def _():
            j = i - 2
            ring_end(rows_in, j, xrecv)
            gate_act = jnp.zeros((span, gate_w.shape[1]), f32)
            up_act = jnp.zeros((span, gate_w.shape[1]), f32)
            squares = jnp.zeros((span, 1), f32)
            for k in range(n_tp):
                values = rows_in[k, whole(j)].astype(f32)
                squares = squares + jnp.sum(values * values, axis=1, keepdims=True)
                block = (values * ffgain_ref[k]).astype(bf16)
                gate_act = gate_act + nn(block, gate_w[k * dcols : (k + 1) * dcols])
                up_act = up_act + nn(block, up_w[k * dcols : (k + 1) * dcols])
            scale = lax.rsqrt(squares / (n_tp * dcols) + EPSILON)
            gate_act = gate_act * scale
            up_act = up_act * scale
            inner[t, whole(j)] = (silu(gate_act) * up_act).astype(bf16)
            ring_start(inner, j, isend, irecv)

        @pl.when((i >= 3) & (i < chunks + 3))
        def _():
            ring_forward(inner, i - 3, isend, irecv)

        @pl.when(i >= 4)
        def _():
            j = i - 4

            @pl.when(j == 0)
            def _():
                own_down.wait()
                for c in down_sends + down_last:
                    c.wait_recv()

            ring_end(inner, j, irecv)
            out = jnp.zeros((span, dcols), f32)
            for k in range(n_tp):
                out = out + nn(
                    inner[k, whole(j)], down_w[k * hidden_units : (k + 1) * hidden_units]
                )
            outs[whole(j)] = out.astype(bf16)

            @pl.loop(0, per_chunk)
            def _(k):
                target = (
                    source_plane(j) * plane_size + plane_half(j)[1] * per_chunk + lax.rem(b_me + k, per_chunk)
                )

                @pl.when(target != me)
                def _():
                    copy_to(
                        outs.at[message(target)],
                        returned.at[message(me)],
                        rsend,
                        rrecv.at[j // early],
                        {"sp": target},
                    ).start()

    returned[message(me)] = outs[message(me)]
    for c in shares:
        c.wait_recv()
    eye = (
        lax.broadcasted_iota(jnp.int32, (quarter, 128), 0) == lax.broadcasted_iota(jnp.int32, (quarter, 128), 1)
    ).astype(bf16)
    shares_of = []
    for k in range(n_tp):
        p_hi, p_mid, p_lo = split3(router[k])
        shares_of.append(nt(eye, p_hi) + nt(eye, p_mid) + nt(eye, p_lo))
    share = jnp.concatenate(shares_of, axis=0)
    total = resid_ref[...]
    wait_bytes(returned.at[pl.ds(0, early * span - 16)], rrecv.at[0])
    for i in range(planes):
        if i == early // 2:
            wait_bytes(returned.at[pl.ds(0, (chunks - early) * span)], rrecv.at[1])
        there = lax.rem(z + offset(i), planes)
        block = pl.ds(pl.multiple_of(there * 2 * span, 2 * span), 2 * span)
        values = returned[block]
        for j in range(TOPK):
            total = total + share[:, j : j + 1] * nn(from_slots[j, :, block], values)
    slices[...] = total.astype(bf16)
    def columns_of(k):
        return pl.ds(pl.multiple_of(k * dcols, dcols), dcols)

    def slice_of(k):
        return slices.at[pl.ds(pl.multiple_of(k * quarter, quarter), quarter)]

    last = [
        copy_to(slice_of(other), out_ref.at[:, columns_of(t)], fsend.at[k], frecv.at[k], {"tp": other})
        for k, other in enumerate((opposite, right, left))
    ]
    for c in last:
        c.start()
    own_out = pltpu.make_async_copy(slice_of(t), out_ref.at[:, columns_of(t)], osem)
    own_out.start()
    own_out.wait()
    for c in last:
        c.wait_recv()
    for c in last + shares + down_sends + down_relay + down_last:
        c.wait_send()
    wait_bytes(sendbuf.at[pl.ds(0, slots - 16)], zsend)
    wait_bytes(outs.at[pl.ds(0, slots - 16)], rsend)
    wait_bytes(rows_in.at[pl.ds(0, 3)], xsend)
    wait_bytes(inner.at[pl.ds(0, 3)], isend)
    for c in to_right + to_left + [on_right, on_left]:
        c.wait_send()

    @pl.when(is_owner)
    def _():
        wait_bytes(msg.at[pl.ds(0, OWNERS - 1)], msend)
        wait_bytes(carr.at[pl.ds(0, n_sp - 1)], bsend)

    @pl.when(jnp.logical_not(is_owner))
    def _():
        wait_bytes(msg.at[pl.ds(0, OWNERS)], msend)


def per_device(
    query, forget, value, gate, fmin, eld, gain, wout, stream, ffgain, routes, router,
    gate_weight, up_weight, down_weight,
):
    rows, width = query.shape
    n_sp, n_tp = lax.axis_size("sp"), lax.axis_size("tp")
    model = stream.shape[1]
    dcols = model // n_tp
    slots = n_sp * 16
    units = down_weight.shape[1]
    vmem = pl.BlockSpec(memory_space=pltpu.VMEM)
    hbm = pl.BlockSpec(memory_space=pl.ANY)
    dma = pltpu.SemaphoreType.DMA
    return pl.pallas_call(
        layer_kernel,
        name="layer",
        out_shape=jax.ShapeDtypeStruct(stream.shape, bf16),
        in_specs=[hbm] * 4 + [vmem] * 3 + [hbm, hbm] + [vmem] * 3 + [hbm] * 3,
        out_specs=hbm,
        scratch_shapes=[
            pltpu.VMEM((rows, width), bf16),
            pltpu.VMEM((rows, width), bf16),
            pltpu.VMEM((rows, width), bf16),
            pltpu.VMEM((rows, width), bf16),
            pltpu.VMEM(wout.shape, bf16),
            pltpu.VMEM((rows, dcols), bf16),
            pltpu.VMEM((OWNERS, 16, 128), bf16),
            pltpu.VMEM((n_sp, 16, 128), bf16),
            pltpu.VMEM((n_sp, 8, 128), bf16),
            pltpu.VMEM((OWNERS, 8, 128), bf16),
            pltpu.VMEM((rows, width), f32),
            pltpu.VMEM((rows, width), bf16),
            pltpu.VMEM((rows, width), bf16),
            pltpu.VMEM((n_tp, rows, width), bf16),
            pltpu.VMEM((rows, dcols), f32),
            pltpu.VMEM((model, units), bf16),
            pltpu.VMEM((model, units), bf16),
            pltpu.VMEM((n_tp * units, dcols), bf16),
            pltpu.VMEM((2, units // 2, dcols), bf16),
            pltpu.VMEM((slots, rows), bf16),
            pltpu.VMEM((TOPK, rows, slots), bf16),
            pltpu.VMEM((n_tp, 8, 128), f32),
            pltpu.VMEM((slots, dcols), bf16),
            pltpu.VMEM((n_tp, slots, dcols), bf16),
            pltpu.VMEM((n_tp, slots, units), bf16),
            pltpu.VMEM((slots, dcols), bf16),
            pltpu.VMEM((slots, dcols), bf16),
            pltpu.VMEM((rows, dcols), bf16),
            dma, dma, dma, dma, dma, dma((6,)), dma((6,)), dma((3,)), dma((3,)), dma,
            dma, dma, dma, dma((6,)), dma((6,)), dma((3,)), dma((3,)),
            dma, dma((16,)), dma, dma((16, 2)), dma, dma((16, 2)), dma, dma((2,)), dma((3,)), dma((3,)), dma((4,)), dma,
        ],
        compiler_params=pltpu.CompilerParams(
            collective_id=0, has_side_effects=True, vmem_limit_bytes=LIMIT * 2**20
        ),
    )(
        query, forget, value, gate, fmin, eld, gain, wout, stream,
        ffgain.reshape(n_tp, 1, dcols), routes.T, router.T, gate_weight, up_weight, down_weight,
    )


def solution(mesh):
    both = ("sp", "tp")
    placed = (
        P("sp", "tp"), P("sp", "tp"), P("sp", "tp"), P("sp", "tp"), P("tp"), P("tp", "sp"), P("tp"),
        P(None, "tp"), P(both, None), P(), P("sp", None), P(both, None),
        P("sp", None, "tp"), P("sp", None, "tp"), P("sp", "tp", None),
    )
    return jax.shard_map(
        per_device, mesh=mesh, in_specs=placed, out_specs=P(both, None), check_vma=False
    )
```

```python
import jax
import jax.numpy as jnp
from jax import lax
from jax.experimental import pallas as pl
from jax.experimental.pallas import tpu as pltpu
from jax.sharding import PartitionSpec as P

TOPK = 2
EPSILON = 1e-06
OWNERS = 48
LIMIT = 56
PLANE_ORDER = sum(offset * 8**k for k, offset in enumerate((0, 7, 2, 5, 4, 3, 6, 1)))
MESH = pl.DeviceIdType.MESH
f32 = jnp.float32
bf16 = jnp.bfloat16


def nn(a, b):
    return jnp.dot(a, b, preferred_element_type=f32)


def nt(a, b):
    return lax.dot_general(a, b, (((1,), (1,)), ((), ())), preferred_element_type=f32)


def tn(a, b):
    return lax.dot_general(a, b, (((0,), (0,)), ((), ())), preferred_element_type=f32)


def split2(x):
    hi = x.astype(bf16)
    return hi, (x - hi.astype(f32)).astype(bf16)


def split3(x):
    hi = x.astype(bf16)
    rest = x - hi.astype(f32)
    mid = rest.astype(bf16)
    return hi, mid, (rest - mid.astype(f32)).astype(bf16)


def sigmoid(x):
    return 1.0 / (1.0 + jnp.exp(-x))


def silu(x):
    return x / (1.0 + jnp.exp(-x))


def copy_to(src, dst, send, recv, target):
    return pltpu.make_async_remote_copy(
        src_ref=src, dst_ref=dst, send_sem=send, recv_sem=recv, device_id=target, device_id_type=MESH
    )


def wait_bytes(ref, sem):
    pltpu.make_async_copy(ref, ref, sem).wait()


def layer_kernel(
    q_hbm, f_hbm, v_hbm, g_hbm, fmin_ref, eld_ref, gain_ref, wout_hbm, stream_hbm, ffgain_ref,
    routes_ref, router_ref, gate_hbm, up_hbm, down_hbm,
    out_ref,
    q_ref, f_ref, v_ref, g_ref, wout, strm, msg, got, carr, back, acc, qe_hi, qe_lo, hid, resid_ref,
    gate_w, up_w, down_w, relay, to_slots, from_slots, router, sendbuf, rows_in, inner, outs, returned, slices,
    wsem, msend, mrecv, bsend, brecv, hsend, hrecv, tsend, trecv, lsem,
    gsem, usem, dsem, dsend, drecv, psend, precv, zsend, zrecv, xsend, xrecv, isend, irecv,
    rsend, rrecv, fsend, frecv, insem, osem,
):
    rows = q_ref.shape[0]
    half = rows // 2
    heads = q_ref.shape[1] // 128
    me = lax.axis_index("sp")
    t = lax.axis_index("tp")
    n_sp = lax.axis_size("sp")
    n_tp = lax.axis_size("tp")
    right, left = lax.rem(t + 1, n_tp), lax.rem(t + n_tp - 1, n_tp)
    opposite = lax.rem(t + 2, n_tp)
    dcols = resid_ref.shape[1]
    quarter = rows // n_tp
    width = q_ref.shape[1]

    loads = [
        pltpu.make_async_copy(src, dst, insem.at[i])
        for i, (src, dst) in enumerate(((f_hbm, f_ref), (v_hbm, v_ref), (q_hbm, q_ref), (g_hbm, g_ref)))
    ]
    for c in loads:
        c.start()

    barrier = pltpu.get_barrier_semaphore()

    @pl.loop(1, n_sp)
    def _(k):
        pl.semaphore_signal(barrier, inc=1, device_id={"sp": lax.rem(me + k, n_sp)}, device_id_type=MESH)

    for k in range(1, n_tp):
        pl.semaphore_signal(barrier, inc=1, device_id={"tp": lax.rem(t + k, n_tp)}, device_id_type=MESH)

    weight_copy = pltpu.make_async_copy(wout_hbm, wout, wsem)
    weight_copy.start()
    own_rows = pl.ds(pl.multiple_of(t * quarter, quarter), quarter)
    own_stream = pltpu.make_async_copy(
        stream_hbm.at[:, pl.ds(pl.multiple_of(t * dcols, dcols), dcols)], strm.at[own_rows], lsem
    )
    own_stream.start()
    gate_copy = pltpu.make_async_copy(gate_hbm.at[0], gate_w, gsem)
    up_copy = pltpu.make_async_copy(up_hbm.at[0], up_w, usem)
    gate_copy.start()
    up_copy.start()
    hidden_units = down_hbm.shape[1]
    own_units = pl.ds(pl.multiple_of(t * hidden_units, hidden_units), hidden_units)

    def down_part(k):
        return down_hbm.at[0, :, pl.ds(pl.multiple_of(k * dcols, dcols), dcols)]

    own_down = pltpu.make_async_copy(down_part(t), down_w.at[own_units], dsem)
    own_down.start()
    picked = router_ref[...] / (router_ref[0:1] + router_ref[1:2])
    router[t] = jnp.zeros((8, 128), f32)
    router[t, 0:TOPK, 0:quarter] = picked

    lower = (
        lax.broadcasted_iota(jnp.int32, (rows, rows), 0) >= lax.broadcasted_iota(jnp.int32, (rows, rows), 1)
    ).astype(bf16)
    loads[0].wait()
    weight = (1.0 - fmin_ref[...].reshape(1, width)) * sigmoid(-f_ref[...].astype(f32))
    d_hi, d_mid, d_lo = split3(jnp.log1p(-weight))
    decay = nn(lower, d_hi) + nn(lower, d_mid) + nn(lower, d_lo)
    e_hi, e_mid, e_lo = split3(eld_ref[...])
    extra = nt(lower, e_hi) + nt(lower, e_mid) + nt(lower, e_lo)

    loads[1].wait()
    row_of = lax.broadcasted_iota(jnp.int32, (8, 128), 0)
    parts = []
    for h in range(heads):
        lanes = slice(h * 128, (h + 1) * 128)
        run = decay[:, lanes] + extra[:, h : h + 1]
        w_h = weight[:, lanes]
        mid, end = run[half - 1 : half], run[rows - 1 : rows]
        v0, v1 = v_ref[0:half, lanes], v_ref[half:rows, lanes]
        k0_hi, k0_lo = split2(w_h[0:half] * jnp.exp(mid - run[0:half]))
        k1_hi, k1_lo = split2(w_h[half:rows] * jnp.exp(end - run[half:rows]))
        s0 = tn(v0, k0_hi) + tn(v0, k0_lo)
        s1 = tn(v1, k1_hi) + tn(v1, k1_lo)
        local = jnp.exp(end - mid) * s0 + s1
        t_hi, t_mid, t_lo = split3(end)
        tail = jnp.where(
            row_of == 0,
            t_hi.astype(f32),
            jnp.where(row_of == 1, t_mid.astype(f32), jnp.where(row_of == 2, t_lo.astype(f32), 0.0)),
        )
        piece = jnp.concatenate(
            [local.reshape(16, 8, 128), jnp.broadcast_to(tail[None], (16, 8, 128))], axis=1
        )
        msg[h * 16 : (h + 1) * 16] = piece.astype(bf16)
        parts.append((run, w_h, v0, v1, mid, s0))

    pl.semaphore_wait(barrier, n_sp + n_tp - 2)

    def owner_device(p):
        return (p // 3) * 4 + lax.rem(p, 3)

    is_owner = lax.rem(me, 4) < 3
    mine = (me // 4) * 3 + jnp.minimum(lax.rem(me, 4), 2)

    plane_size = 8
    planes = n_sp // plane_size
    per_plane = OWNERS // planes
    z = me // plane_size
    b_me = lax.rem(me, plane_size)
    far_first = (4, 3, 5, 2, 6, 1, 7, 0)
    for away in far_first:

        @pl.loop(0, per_plane)
        def _(k, away=away):
            p = lax.rem(z + away, planes) * per_plane + lax.rem(b_me + k, per_plane)
            target = owner_device(p)

            @pl.when(target != me)
            def _():
                copy_to(msg.at[p], got.at[me], msend, mrecv, {"sp": target}).start()

    for k in range(1, n_tp):
        other = lax.rem(t + k, n_tp)
        copy_to(
            stream_hbm.at[:, pl.ds(pl.multiple_of(other * dcols, dcols), dcols)],
            strm.at[own_rows],
            tsend.at[k - 1],
            trecv.at[k - 1],
            {"tp": other},
        ).start()
    shares = [
        copy_to(router.at[t], router.at[t], psend.at[k - 1], precv.at[k - 1], {"tp": lax.rem(t + k, n_tp)})
        for k in range(1, n_tp)
    ]
    for c in shares:
        c.start()

    unit_half = hidden_units // 2
    down_sends = [
        copy_to(down_part(other), down_w.at[own_units], dsend.at[k], drecv.at[k], {"tp": other})
        for k, other in enumerate((right, left))
    ]
    down_sends[0].start()
    down_sends[1].start()
    slots = n_sp * 16
    unit = (
        lax.broadcasted_iota(jnp.int32, (rows, rows), 0) == lax.broadcasted_iota(jnp.int32, (rows, rows), 1)
    ).astype(bf16)
    first = lax.broadcasted_iota(jnp.int32, (rows, rows), 0)
    second = lax.broadcasted_iota(jnp.int32, (rows, rows), 1)
    same = (first >> 6) == (second >> 6)
    earlier = ((first < second) & same).astype(bf16)
    later = ((second < first) & same).astype(bf16)
    routes = routes_ref[...]
    slot = lax.broadcasted_iota(jnp.int32, (slots, rows), 0)
    token = lax.broadcasted_iota(jnp.int32, (slots, rows), 1)
    named = (routes[0:1] == (slot >> 4)) | (routes[1:2] == (slot >> 4))
    count = nn(named.astype(bf16), earlier)
    here = named & (count == (slot & 3).astype(f32)) & (((slot >> 2) & 3) == (token >> 6))
    to_slots[...] = here.astype(bf16)
    columns = nt(unit, routes.astype(f32).astype(bf16))
    slot = lax.broadcasted_iota(jnp.int32, (rows, slots), 1)
    token = lax.broadcasted_iota(jnp.int32, (rows, slots), 0)
    expert = (slot >> 4).astype(f32)
    chosen = [columns[:, j : j + 1] == expert for j in range(TOPK)]
    count = nn(later, (chosen[0] | chosen[1]).astype(bf16))
    fits = (count == (slot & 3).astype(f32)) & (((slot >> 2) & 3) == (token >> 6))
    for j in range(TOPK):
        from_slots[j] = (chosen[j] & fits).astype(bf16)

    loads[2].wait()
    causal = lax.broadcasted_iota(jnp.int32, (half, half), 0) >= lax.broadcasted_iota(
        jnp.int32, (half, half), 1
    )
    for h in range(heads):
        lanes = slice(h * 128, (h + 1) * 128)
        run, w_h, v0, v1, mid, s0 = parts[h]
        query = silu(q_ref[:, lanes].astype(f32))
        full_hi, full_lo = split2(query * jnp.exp(run))
        qe_hi[:, lanes] = full_hi
        qe_lo[:, lanes] = full_lo
        for c, values in ((0, v0), (1, v1)):
            span = slice(c * half, (c + 1) * half)
            centre = run[c * half + half // 2 - 1 : c * half + half // 2]
            a_hi, a_lo = split2(query[span] * jnp.exp(run[span] - centre))
            b_hi, b_lo = split2(w_h[span] * jnp.exp(centre - run[span]))
            scores = nt(a_hi, b_hi) + nt(a_hi, b_lo) + nt(a_lo, b_hi)
            p_hi, p_lo = split2(jnp.where(causal, scores, 0.0))
            out = nn(p_hi, values) + nn(p_lo, values)
            if c == 1:
                c_hi, c_lo = split2(query[span] * jnp.exp(run[span] - mid))
                z_hi, z_lo = split2(s0)
                out = out + nt(c_hi, z_hi) + nt(c_hi, z_lo) + nt(c_lo, z_hi)
            acc[span, lanes] = out

    @pl.when(is_owner)
    def _():
        got[me] = msg[mine]
        wait_bytes(got.at[pl.ds(0, n_sp - 1)], mrecv)

        def step(i, state):
            carr[i] = state.astype(bf16)
            block = got[i].astype(f32)
            total = block[8:9] + block[9:10] + block[10:11]
            return jnp.exp(total) * state + block[0:8]

        lax.fori_loop(0, n_sp, step, jnp.zeros((8, 128), f32), unroll=8)
        back[mine] = carr[me]

        for away in far_first:

            @pl.loop(0 if away else 1, plane_size)
            def _(k, away=away):
                target = lax.rem(z + away, planes) * plane_size + lax.rem(b_me + k, plane_size)
                copy_to(carr.at[target], back.at[mine], bsend, brecv, {"sp": target}).start()

    loads[3].wait()
    gate = gain_ref[...].reshape(1, width) * silu(g_ref[...].astype(f32))

    @pl.when(is_owner)
    def _():
        wait_bytes(back.at[pl.ds(0, OWNERS - 1)], brecv)

    @pl.when(jnp.logical_not(is_owner))
    def _():
        wait_bytes(back.at[pl.ds(0, OWNERS)], brecv)

    for h in range(heads):
        lanes = slice(h * 128, (h + 1) * 128)
        state = back[h * 16 : (h + 1) * 16].astype(f32).reshape(128, 128).astype(bf16)
        out = acc[:, lanes] + nt(qe_hi[:, lanes], state) + nt(qe_lo[:, lanes], state)
        out = out * lax.rsqrt(jnp.mean(out * out, axis=1, keepdims=True) + EPSILON)
        hid[t, :, lanes] = (out * gate[:, lanes]).astype(bf16)

    top, low = pl.ds(0, half), pl.ds(half, half)
    to_right = [
        copy_to(hid.at[t, r], hid.at[t, r], hsend.at[i], hrecv.at[i], {"tp": right})
        for i, r in enumerate((top, low))
    ]
    to_left = [
        copy_to(hid.at[t, r], hid.at[t, r], hsend.at[2 + i], hrecv.at[2 + i], {"tp": left})
        for i, r in enumerate((low, top))
    ]
    to_right[0].start()
    to_left[0].start()
    to_right[1].start()
    to_left[1].start()
    weight_copy.wait()

    def partial(block):
        return nn(hid[block], wout[pl.ds(pl.multiple_of(block * width, width), width), :])

    proj = partial(t)
    to_right[0].wait_recv()
    on_right = copy_to(hid.at[left, top], hid.at[left, top], hsend.at[4], hrecv.at[4], {"tp": right})
    on_right.start()
    to_left[0].wait_recv()
    on_left = copy_to(hid.at[right, low], hid.at[right, low], hsend.at[5], hrecv.at[5], {"tp": left})
    on_left.start()
    down_relay = [
        copy_to(
            down_hbm.at[0, pl.ds(s * unit_half, unit_half), pl.ds(pl.multiple_of(opposite * dcols, dcols), dcols)],
            relay.at[s],
            dsend.at[2 + s],
            drecv.at[2 + s],
            {"tp": other},
        )
        for s, other in ((0, right), (1, left))
    ]
    down_relay[0].start()
    down_relay[1].start()
    to_right[1].wait_recv()
    proj = proj + partial(left)
    to_left[1].wait_recv()
    proj = proj + partial(right)
    own_stream.wait()
    for k in range(1, n_tp):
        other = lax.rem(t + k, n_tp)
        copy_to(
            stream_hbm.at[:, pl.ds(pl.multiple_of(other * dcols, dcols), dcols)],
            strm.at[own_rows],
            tsend.at[k - 1],
            trecv.at[k - 1],
            {"tp": other},
        ).wait()
    on_right.wait_recv()
    on_left.wait_recv()
    proj = proj + partial(opposite)
    resid = strm[...].astype(f32) + proj.astype(bf16).astype(f32)
    resid_ref[...] = resid
    rounded = resid.astype(bf16)

    chunks = 2 * planes
    per_chunk = plane_size // 2
    span, part = per_chunk * 16, per_chunk * 8
    my_half = b_me % 2
    my_place = z * plane_size + my_half * per_chunk + b_me // 2

    def message(k):
        return pl.ds(pl.multiple_of(k * 16, 16), 16)

    def offset(plane):
        power = (1 + 7 * (plane % 2)) * (1 + 63 * ((plane // 2) % 2)) * (1 + 4095 * (plane // 4))
        return (PLANE_ORDER // power) % 8

    def plane_half(i):
        last = i // (chunks - 4)
        plane = (1 - last) * (i // 2) + last * (planes - 2 + i % 2)
        return plane, (1 - last) * (i % 2) + last * ((i // 2) % 2)

    def source_plane(i):
        return lax.rem(z + planes - offset(plane_half(i)[0]), planes)

    def chunk(i):
        return (source_plane(i) * 2 + plane_half(i)[1]) * span

    def whole(i):
        return pl.ds(pl.multiple_of(chunk(i), span), span)

    def piece(i, s):
        return pl.ds(pl.multiple_of(chunk(i) + s * part, part), part)

    for i in range(planes):
        there = lax.rem(z + offset(i), planes)
        block = pl.ds(pl.multiple_of(there * 2 * span, 2 * span), 2 * span)
        sendbuf[block] = nn(to_slots[block], rounded).astype(bf16)

        @pl.loop(1 if i == 0 else 0, plane_size)
        def _(k, i=i, there=there):
            target = there * plane_size + lax.rem(b_me + k, plane_size)
            copy_to(
                sendbuf.at[message(target)],
                rows_in.at[t, message(my_place)],
                zsend,
                zrecv.at[2 * i + my_half],
                {"sp": target},
            ).start()

    rows_in[t, message(my_place)] = sendbuf[message(me)]
    down_last = [
        copy_to(
            relay.at[s],
            down_w.at[pl.ds(pl.multiple_of(source * hidden_units + s * unit_half, unit_half), unit_half)],
            dsend.at[4 + s],
            drecv.at[4 + s],
            {"tp": target},
        )
        for s, source, target in ((0, left, right), (1, right, left))
    ]
    for s in range(2):
        down_relay[s].wait_recv()
        down_last[s].start()
    gate_copy.wait()
    up_copy.wait()

    early = chunks - 4

    def ring_start(ref, i, send, recv, direct):
        for s, target, n in ((0, right, 0), (1, left, 0), (1, right, 1), (0, left, 1)):
            here = ref.at[t, piece(i, s)]
            copy_to(here, here, send, recv.at[i, n], {"tp": target}).start()

        @pl.when(i >= direct)
        def _():
            here = ref.at[t, whole(i)]
            copy_to(here, here, send, recv.at[i, 1], {"tp": opposite}).start()

    def ring_forward(ref, i, send, recv, direct):
        wait_bytes(ref.at[t, whole(i)], recv.at[i, 0])

        @pl.when(i < direct)
        def _():
            for s, source, target in ((0, left, right), (1, right, left)):
                here = ref.at[source, piece(i, s)]
                copy_to(here, here, send, recv.at[i, 1], {"tp": target}).start()

    def ring_end(ref, i, recv):
        wait_bytes(ref.at[t, pl.ds(0, 2 * span)], recv.at[i, 1])

    @pl.loop(0, chunks + 4)
    def _(i):
        @pl.when(i < chunks)
        def _():
            plane, half_of = plane_half(i)
            arrival = zrecv.at[2 * plane + half_of]
            local = (plane == 0) & (half_of == my_half)

            @pl.when(local)
            def _():
                wait_bytes(rows_in.at[t, pl.ds(0, span - 16)], arrival)

            @pl.when(jnp.logical_not(local))
            def _():
                wait_bytes(rows_in.at[t, whole(i)], arrival)

            ring_start(rows_in, i, xsend, xrecv, chunks)

        @pl.when((i >= 1) & (i < chunks + 1))
        def _():
            ring_forward(rows_in, i - 1, xsend, xrecv, chunks)

        @pl.when((i >= 2) & (i < chunks + 2))
        def _():
            j = i - 2
            ring_end(rows_in, j, xrecv)
            gate_act = jnp.zeros((span, gate_w.shape[1]), f32)
            up_act = jnp.zeros((span, gate_w.shape[1]), f32)
            squares = jnp.zeros((span, 1), f32)
            for k in range(n_tp):
                values = rows_in[k, whole(j)].astype(f32)
                squares = squares + jnp.sum(values * values, axis=1, keepdims=True)
                block = (values * ffgain_ref[k]).astype(bf16)
                gate_act = gate_act + nn(block, gate_w[k * dcols : (k + 1) * dcols])
                up_act = up_act + nn(block, up_w[k * dcols : (k + 1) * dcols])
            scale = lax.rsqrt(squares / (n_tp * dcols) + EPSILON)
            gate_act = gate_act * scale
            up_act = up_act * scale
            inner[t, whole(j)] = (silu(gate_act) * up_act).astype(bf16)
            ring_start(inner, j, isend, irecv, chunks - 1)

        @pl.when((i >= 3) & (i < chunks + 3))
        def _():
            ring_forward(inner, i - 3, isend, irecv, chunks - 1)

        @pl.when(i >= 4)
        def _():
            j = i - 4

            @pl.when(j == 0)
            def _():
                own_down.wait()
                for c in down_sends + down_last:
                    c.wait_recv()

            ring_end(inner, j, irecv)
            out = jnp.zeros((span, dcols), f32)
            for k in range(n_tp):
                out = out + nn(
                    inner[k, whole(j)], down_w[k * hidden_units : (k + 1) * hidden_units]
                )
            outs[whole(j)] = out.astype(bf16)

            @pl.loop(0, per_chunk)
            def _(k):
                y = lax.rem(b_me // 2 + k, per_chunk)
                target = source_plane(j) * plane_size + 2 * y + plane_half(j)[1]

                @pl.when(target != me)
                def _():
                    copy_to(
                        outs.at[pl.ds(pl.multiple_of(chunk(j) + y * 16, 16), 16)],
                        returned.at[message(me)],
                        rsend,
                        rrecv.at[j // early],
                        {"sp": target},
                    ).start()

    returned[message(me)] = outs[message(my_place)]
    for c in shares:
        c.wait_recv()
    eye = (
        lax.broadcasted_iota(jnp.int32, (quarter, 128), 0) == lax.broadcasted_iota(jnp.int32, (quarter, 128), 1)
    ).astype(bf16)
    shares_of = []
    for k in range(n_tp):
        p_hi, p_mid, p_lo = split3(router[k])
        shares_of.append(nt(eye, p_hi) + nt(eye, p_mid) + nt(eye, p_lo))
    share = jnp.concatenate(shares_of, axis=0)
    total = resid_ref[...]
    wait_bytes(returned.at[pl.ds(0, early * span - 16)], rrecv.at[0])
    for i in range(planes):
        if i == early // 2:
            wait_bytes(returned.at[pl.ds(0, (chunks - early) * span)], rrecv.at[1])
        there = lax.rem(z + offset(i), planes)
        block = pl.ds(pl.multiple_of(there * 2 * span, 2 * span), 2 * span)
        values = returned[block]
        for j in range(TOPK):
            total = total + share[:, j : j + 1] * nn(from_slots[j, :, block], values)
    slices[...] = total.astype(bf16)
    def columns_of(k):
        return pl.ds(pl.multiple_of(k * dcols, dcols), dcols)

    def slice_of(k):
        return slices.at[pl.ds(pl.multiple_of(k * quarter, quarter), quarter)]

    last = [
        copy_to(slice_of(other), out_ref.at[:, columns_of(t)], fsend.at[k], frecv.at[k], {"tp": other})
        for k, other in enumerate((opposite, right, left))
    ]
    for c in last:
        c.start()
    own_out = pltpu.make_async_copy(slice_of(t), out_ref.at[:, columns_of(t)], osem)
    own_out.start()
    own_out.wait()
    for c in last:
        c.wait_recv()
    for c in last + shares + down_sends + down_relay + down_last:
        c.wait_send()
    wait_bytes(sendbuf.at[pl.ds(0, slots - 16)], zsend)
    wait_bytes(outs.at[pl.ds(0, slots - 16)], rsend)
    wait_bytes(rows_in.at[pl.ds(0, 3)], xsend)
    wait_bytes(inner.at[pl.ds(0, 3)], isend)
    for c in to_right + to_left + [on_right, on_left]:
        c.wait_send()

    @pl.when(is_owner)
    def _():
        wait_bytes(msg.at[pl.ds(0, OWNERS - 1)], msend)
        wait_bytes(carr.at[pl.ds(0, n_sp - 1)], bsend)

    @pl.when(jnp.logical_not(is_owner))
    def _():
        wait_bytes(msg.at[pl.ds(0, OWNERS)], msend)


def per_device(
    query, forget, value, gate, fmin, eld, gain, wout, stream, ffgain, routes, router,
    gate_weight, up_weight, down_weight,
):
    rows, width = query.shape
    n_sp, n_tp = lax.axis_size("sp"), lax.axis_size("tp")
    model = stream.shape[1]
    dcols = model // n_tp
    slots = n_sp * 16
    units = down_weight.shape[1]
    vmem = pl.BlockSpec(memory_space=pltpu.VMEM)
    hbm = pl.BlockSpec(memory_space=pl.ANY)
    dma = pltpu.SemaphoreType.DMA
    return pl.pallas_call(
        layer_kernel,
        name="layer",
        out_shape=jax.ShapeDtypeStruct(stream.shape, bf16),
        in_specs=[hbm] * 4 + [vmem] * 3 + [hbm, hbm] + [vmem] * 3 + [hbm] * 3,
        out_specs=hbm,
        scratch_shapes=[
            pltpu.VMEM((rows, width), bf16),
            pltpu.VMEM((rows, width), bf16),
            pltpu.VMEM((rows, width), bf16),
            pltpu.VMEM((rows, width), bf16),
            pltpu.VMEM(wout.shape, bf16),
            pltpu.VMEM((rows, dcols), bf16),
            pltpu.VMEM((OWNERS, 16, 128), bf16),
            pltpu.VMEM((n_sp, 16, 128), bf16),
            pltpu.VMEM((n_sp, 8, 128), bf16),
            pltpu.VMEM((OWNERS, 8, 128), bf16),
            pltpu.VMEM((rows, width), f32),
            pltpu.VMEM((rows, width), bf16),
            pltpu.VMEM((rows, width), bf16),
            pltpu.VMEM((n_tp, rows, width), bf16),
            pltpu.VMEM((rows, dcols), f32),
            pltpu.VMEM((model, units), bf16),
            pltpu.VMEM((model, units), bf16),
            pltpu.VMEM((n_tp * units, dcols), bf16),
            pltpu.VMEM((2, units // 2, dcols), bf16),
            pltpu.VMEM((slots, rows), bf16),
            pltpu.VMEM((TOPK, rows, slots), bf16),
            pltpu.VMEM((n_tp, 8, 128), f32),
            pltpu.VMEM((slots, dcols), bf16),
            pltpu.VMEM((n_tp, slots, dcols), bf16),
            pltpu.VMEM((n_tp, slots, units), bf16),
            pltpu.VMEM((slots, dcols), bf16),
            pltpu.VMEM((slots, dcols), bf16),
            pltpu.VMEM((rows, dcols), bf16),
            dma, dma, dma, dma, dma, dma((6,)), dma((6,)), dma((3,)), dma((3,)), dma,
            dma, dma, dma, dma((6,)), dma((6,)), dma((3,)), dma((3,)),
            dma, dma((16,)), dma, dma((16, 2)), dma, dma((16, 2)), dma, dma((2,)), dma((3,)), dma((3,)), dma((4,)), dma,
        ],
        compiler_params=pltpu.CompilerParams(
            collective_id=0, has_side_effects=True, vmem_limit_bytes=LIMIT * 2**20
        ),
    )(
        query, forget, value, gate, fmin, eld, gain, wout, stream,
        ffgain.reshape(n_tp, 1, dcols), routes.T, router.T, gate_weight, up_weight, down_weight,
    )


def solution(mesh):
    both = ("sp", "tp")
    placed = (
        P("sp", "tp"), P("sp", "tp"), P("sp", "tp"), P("sp", "tp"), P("tp"), P("tp", "sp"), P("tp"),
        P(None, "tp"), P(both, None), P(), P("sp", None), P(both, None),
        P("sp", None, "tp"), P("sp", None, "tp"), P("sp", "tp", None),
    )
    return jax.shard_map(
        per_device, mesh=mesh, in_specs=placed, out_specs=P(both, None), check_vma=False
    )
```

```python
import jax
import jax.numpy as jnp
from jax import lax
from jax.experimental import pallas as pl
from jax.experimental.pallas import tpu as pltpu
from jax.sharding import PartitionSpec as P

TOPK = 2
EPSILON = 1e-06
OWNERS = 48
LIMIT = 56
PLANE_ORDER = sum(offset * 8**k for k, offset in enumerate((0, 7, 2, 5, 4, 3, 6, 1)))
MESH = pl.DeviceIdType.MESH
f32 = jnp.float32
bf16 = jnp.bfloat16


def nn(a, b):
    return jnp.dot(a, b, preferred_element_type=f32)


def nt(a, b):
    return lax.dot_general(a, b, (((1,), (1,)), ((), ())), preferred_element_type=f32)


def tn(a, b):
    return lax.dot_general(a, b, (((0,), (0,)), ((), ())), preferred_element_type=f32)


def split2(x):
    hi = x.astype(bf16)
    return hi, (x - hi.astype(f32)).astype(bf16)


def split3(x):
    hi = x.astype(bf16)
    rest = x - hi.astype(f32)
    mid = rest.astype(bf16)
    return hi, mid, (rest - mid.astype(f32)).astype(bf16)


def sigmoid(x):
    return 1.0 / (1.0 + jnp.exp(-x))


def silu(x):
    return x / (1.0 + jnp.exp(-x))


def copy_to(src, dst, send, recv, target):
    return pltpu.make_async_remote_copy(
        src_ref=src, dst_ref=dst, send_sem=send, recv_sem=recv, device_id=target, device_id_type=MESH
    )


def wait_bytes(ref, sem):
    pltpu.make_async_copy(ref, ref, sem).wait()


def layer_kernel(
    q_hbm, f_hbm, v_hbm, g_hbm, fmin_ref, eld_ref, gain_ref, wout_hbm, stream_hbm, ffgain_ref,
    routes_ref, router_ref, gate_hbm, up_hbm, down_hbm,
    out_ref,
    q_ref, f_ref, v_ref, g_ref, wout, strm, msg, got, carr, back, acc, qe_hi, qe_lo, hid, resid_ref,
    gate_w, up_w, down_w, relay, to_slots, from_slots, router, sendbuf, rows_in, inner, outs, returned, slices,
    wsem, msend, mrecv, bsend, brecv, hsend, hrecv, tsend, trecv, lsem,
    gsem, usem, dsem, dsend, drecv, psend, precv, zsend, zrecv, xsend, xrecv, isend, irecv,
    rsend, rrecv, fsend, frecv, insem, osem,
):
    rows = q_ref.shape[0]
    half = rows // 2
    heads = q_ref.shape[1] // 128
    me = lax.axis_index("sp")
    t = lax.axis_index("tp")
    n_sp = lax.axis_size("sp")
    n_tp = lax.axis_size("tp")
    right, left = lax.rem(t + 1, n_tp), lax.rem(t + n_tp - 1, n_tp)
    opposite = lax.rem(t + 2, n_tp)
    dcols = resid_ref.shape[1]
    quarter = rows // n_tp
    width = q_ref.shape[1]

    loads = [
        pltpu.make_async_copy(src, dst, insem.at[i])
        for i, (src, dst) in enumerate(((f_hbm, f_ref), (v_hbm, v_ref), (q_hbm, q_ref), (g_hbm, g_ref)))
    ]
    for c in loads:
        c.start()

    barrier = pltpu.get_barrier_semaphore()

    @pl.loop(1, n_sp)
    def _(k):
        pl.semaphore_signal(barrier, inc=1, device_id={"sp": lax.rem(me + k, n_sp)}, device_id_type=MESH)

    for k in range(1, n_tp):
        pl.semaphore_signal(barrier, inc=1, device_id={"tp": lax.rem(t + k, n_tp)}, device_id_type=MESH)

    weight_copy = pltpu.make_async_copy(wout_hbm, wout, wsem)
    weight_copy.start()
    own_rows = pl.ds(pl.multiple_of(t * quarter, quarter), quarter)
    own_stream = pltpu.make_async_copy(
        stream_hbm.at[:, pl.ds(pl.multiple_of(t * dcols, dcols), dcols)], strm.at[own_rows], lsem
    )
    own_stream.start()
    gate_copy = pltpu.make_async_copy(gate_hbm.at[0], gate_w, gsem)
    up_copy = pltpu.make_async_copy(up_hbm.at[0], up_w, usem)
    gate_copy.start()
    up_copy.start()
    hidden_units = down_hbm.shape[1]
    own_units = pl.ds(pl.multiple_of(t * hidden_units, hidden_units), hidden_units)

    def down_part(k):
        return down_hbm.at[0, :, pl.ds(pl.multiple_of(k * dcols, dcols), dcols)]

    own_down = pltpu.make_async_copy(down_part(t), down_w.at[own_units], dsem)
    own_down.start()
    picked = router_ref[...] / (router_ref[0:1] + router_ref[1:2])
    router[t] = jnp.zeros((8, 128), f32)
    router[t, 0:TOPK, 0:quarter] = picked

    lower = (
        lax.broadcasted_iota(jnp.int32, (rows, rows), 0) >= lax.broadcasted_iota(jnp.int32, (rows, rows), 1)
    ).astype(bf16)
    loads[0].wait()
    weight = (1.0 - fmin_ref[...].reshape(1, width)) * sigmoid(-f_ref[...].astype(f32))
    d_hi, d_mid, d_lo = split3(jnp.log1p(-weight))
    decay = nn(lower, d_hi) + nn(lower, d_mid) + nn(lower, d_lo)
    e_hi, e_mid, e_lo = split3(eld_ref[...])
    extra = nt(lower, e_hi) + nt(lower, e_mid) + nt(lower, e_lo)

    loads[1].wait()
    row_of = lax.broadcasted_iota(jnp.int32, (8, 128), 0)
    parts = []
    for h in range(heads):
        lanes = slice(h * 128, (h + 1) * 128)
        run = decay[:, lanes] + extra[:, h : h + 1]
        w_h = weight[:, lanes]
        mid, end = run[half - 1 : half], run[rows - 1 : rows]
        v0, v1 = v_ref[0:half, lanes], v_ref[half:rows, lanes]
        k0_hi, k0_lo = split2(w_h[0:half] * jnp.exp(mid - run[0:half]))
        k1_hi, k1_lo = split2(w_h[half:rows] * jnp.exp(end - run[half:rows]))
        s0 = tn(v0, k0_hi) + tn(v0, k0_lo)
        s1 = tn(v1, k1_hi) + tn(v1, k1_lo)
        local = jnp.exp(end - mid) * s0 + s1
        t_hi, t_mid, t_lo = split3(end)
        tail = jnp.where(
            row_of == 0,
            t_hi.astype(f32),
            jnp.where(row_of == 1, t_mid.astype(f32), jnp.where(row_of == 2, t_lo.astype(f32), 0.0)),
        )
        piece = jnp.concatenate(
            [local.reshape(16, 8, 128), jnp.broadcast_to(tail[None], (16, 8, 128))], axis=1
        )
        msg[h * 16 : (h + 1) * 16] = piece.astype(bf16)
        parts.append((run, w_h, v0, v1, mid, s0))

    pl.semaphore_wait(barrier, n_sp + n_tp - 2)

    def owner_device(p):
        return (p // 3) * 4 + lax.rem(p, 3)

    is_owner = lax.rem(me, 4) < 3
    mine = (me // 4) * 3 + jnp.minimum(lax.rem(me, 4), 2)

    plane_size = 8
    planes = n_sp // plane_size
    per_plane = OWNERS // planes
    z = me // plane_size
    b_me = lax.rem(me, plane_size)
    far_first = (4, 3, 5, 2, 6, 1, 7, 0)
    for away in far_first:

        @pl.loop(0, per_plane)
        def _(k, away=away):
            p = lax.rem(z + away, planes) * per_plane + lax.rem(b_me + k, per_plane)
            target = owner_device(p)

            @pl.when(target != me)
            def _():
                copy_to(msg.at[p], got.at[me], msend, mrecv, {"sp": target}).start()

    for k in range(1, n_tp):
        other = lax.rem(t + k, n_tp)
        copy_to(
            stream_hbm.at[:, pl.ds(pl.multiple_of(other * dcols, dcols), dcols)],
            strm.at[own_rows],
            tsend.at[k - 1],
            trecv.at[k - 1],
            {"tp": other},
        ).start()
    shares = [
        copy_to(router.at[t], router.at[t], psend, precv.at[k - 1], {"tp": lax.rem(t + k, n_tp)})
        for k in range(1, n_tp)
    ]
    for c in shares:
        c.start()

    unit_half = hidden_units // 2
    down_sends = [
        copy_to(down_part(other), down_w.at[own_units], dsend, drecv.at[k], {"tp": other})
        for k, other in enumerate((right, left))
    ]
    down_sends[0].start()
    down_sends[1].start()
    slots = n_sp * 16
    unit = (
        lax.broadcasted_iota(jnp.int32, (rows, rows), 0) == lax.broadcasted_iota(jnp.int32, (rows, rows), 1)
    ).astype(bf16)
    first = lax.broadcasted_iota(jnp.int32, (rows, rows), 0)
    second = lax.broadcasted_iota(jnp.int32, (rows, rows), 1)
    same = (first >> 6) == (second >> 6)
    earlier = ((first < second) & same).astype(bf16)
    later = ((second < first) & same).astype(bf16)
    routes = routes_ref[...]
    slot = lax.broadcasted_iota(jnp.int32, (slots, rows), 0)
    token = lax.broadcasted_iota(jnp.int32, (slots, rows), 1)
    named = (routes[0:1] == (slot >> 4)) | (routes[1:2] == (slot >> 4))
    count = nn(named.astype(bf16), earlier)
    here = named & (count == (slot & 3).astype(f32)) & (((slot >> 2) & 3) == (token >> 6))
    to_slots[...] = here.astype(bf16)
    columns = nt(unit, routes.astype(f32).astype(bf16))
    slot = lax.broadcasted_iota(jnp.int32, (rows, slots), 1)
    token = lax.broadcasted_iota(jnp.int32, (rows, slots), 0)
    expert = (slot >> 4).astype(f32)
    chosen = [columns[:, j : j + 1] == expert for j in range(TOPK)]
    count = nn(later, (chosen[0] | chosen[1]).astype(bf16))
    fits = (count == (slot & 3).astype(f32)) & (((slot >> 2) & 3) == (token >> 6))
    for j in range(TOPK):
        from_slots[j] = (chosen[j] & fits).astype(bf16)

    loads[2].wait()
    causal = lax.broadcasted_iota(jnp.int32, (half, half), 0) >= lax.broadcasted_iota(
        jnp.int32, (half, half), 1
    )
    for h in range(heads):
        lanes = slice(h * 128, (h + 1) * 128)
        run, w_h, v0, v1, mid, s0 = parts[h]
        query = silu(q_ref[:, lanes].astype(f32))
        full_hi, full_lo = split2(query * jnp.exp(run))
        qe_hi[:, lanes] = full_hi
        qe_lo[:, lanes] = full_lo
        for c, values in ((0, v0), (1, v1)):
            span = slice(c * half, (c + 1) * half)
            centre = run[c * half + half // 2 - 1 : c * half + half // 2]
            a_hi, a_lo = split2(query[span] * jnp.exp(run[span] - centre))
            b_hi, b_lo = split2(w_h[span] * jnp.exp(centre - run[span]))
            scores = nt(a_hi, b_hi) + nt(a_hi, b_lo) + nt(a_lo, b_hi)
            p_hi, p_lo = split2(jnp.where(causal, scores, 0.0))
            out = nn(p_hi, values) + nn(p_lo, values)
            if c == 1:
                c_hi, c_lo = split2(query[span] * jnp.exp(run[span] - mid))
                z_hi, z_lo = split2(s0)
                out = out + nt(c_hi, z_hi) + nt(c_hi, z_lo) + nt(c_lo, z_hi)
            acc[span, lanes] = out

    @pl.when(is_owner)
    def _():
        got[me] = msg[mine]
        wait_bytes(got.at[pl.ds(0, n_sp - 1)], mrecv)

        def step(i, state):
            carr[i] = state.astype(bf16)
            block = got[i].astype(f32)
            total = block[8:9] + block[9:10] + block[10:11]
            return jnp.exp(total) * state + block[0:8]

        lax.fori_loop(0, n_sp, step, jnp.zeros((8, 128), f32), unroll=8)
        back[mine] = carr[me]

        for away in far_first:

            @pl.loop(0 if away else 1, plane_size)
            def _(k, away=away):
                target = lax.rem(z + away, planes) * plane_size + lax.rem(b_me + k, plane_size)
                copy_to(carr.at[target], back.at[mine], bsend, brecv, {"sp": target}).start()

    loads[3].wait()
    gate = gain_ref[...].reshape(1, width) * silu(g_ref[...].astype(f32))

    @pl.when(is_owner)
    def _():
        wait_bytes(back.at[pl.ds(0, OWNERS - 1)], brecv)

    @pl.when(jnp.logical_not(is_owner))
    def _():
        wait_bytes(back.at[pl.ds(0, OWNERS)], brecv)

    for h in range(heads):
        lanes = slice(h * 128, (h + 1) * 128)
        state = back[h * 16 : (h + 1) * 16].astype(f32).reshape(128, 128).astype(bf16)
        out = acc[:, lanes] + nt(qe_hi[:, lanes], state) + nt(qe_lo[:, lanes], state)
        out = out * lax.rsqrt(jnp.mean(out * out, axis=1, keepdims=True) + EPSILON)
        hid[t, :, lanes] = (out * gate[:, lanes]).astype(bf16)

    top, low = pl.ds(0, half), pl.ds(half, half)
    to_right = [
        copy_to(hid.at[t, r], hid.at[t, r], hsend, hrecv.at[i], {"tp": right})
        for i, r in enumerate((top, low))
    ]
    to_left = [
        copy_to(hid.at[t, r], hid.at[t, r], hsend, hrecv.at[2 + i], {"tp": left})
        for i, r in enumerate((low, top))
    ]
    to_right[0].start()
    to_left[0].start()
    to_right[1].start()
    to_left[1].start()
    weight_copy.wait()

    def partial(block):
        return nn(hid[block], wout[pl.ds(pl.multiple_of(block * width, width), width), :])

    proj = partial(t)
    to_right[0].wait_recv()
    on_right = copy_to(hid.at[left, top], hid.at[left, top], hsend, hrecv.at[4], {"tp": right})
    on_right.start()
    to_left[0].wait_recv()
    on_left = copy_to(hid.at[right, low], hid.at[right, low], hsend, hrecv.at[5], {"tp": left})
    on_left.start()
    down_relay = [
        copy_to(
            down_hbm.at[0, pl.ds(s * unit_half, unit_half), pl.ds(pl.multiple_of(opposite * dcols, dcols), dcols)],
            relay.at[s],
            dsend,
            drecv.at[2 + s],
            {"tp": other},
        )
        for s, other in ((0, right), (1, left))
    ]
    down_relay[0].start()
    down_relay[1].start()
    to_right[1].wait_recv()
    proj = proj + partial(left)
    to_left[1].wait_recv()
    proj = proj + partial(right)
    own_stream.wait()
    for k in range(1, n_tp):
        other = lax.rem(t + k, n_tp)
        copy_to(
            stream_hbm.at[:, pl.ds(pl.multiple_of(other * dcols, dcols), dcols)],
            strm.at[own_rows],
            tsend.at[k - 1],
            trecv.at[k - 1],
            {"tp": other},
        ).wait()
    on_right.wait_recv()
    on_left.wait_recv()
    proj = proj + partial(opposite)
    resid = strm[...].astype(f32) + proj.astype(bf16).astype(f32)
    resid_ref[...] = resid
    rounded = resid.astype(bf16)

    chunks = 2 * planes
    per_chunk = plane_size // 2
    span, part = per_chunk * 16, per_chunk * 8
    my_half = b_me % 2
    my_place = z * plane_size + my_half * per_chunk + b_me // 2

    def message(k):
        return pl.ds(pl.multiple_of(k * 16, 16), 16)

    def offset(plane):
        power = (1 + 7 * (plane % 2)) * (1 + 63 * ((plane // 2) % 2)) * (1 + 4095 * (plane // 4))
        return (PLANE_ORDER // power) % 8

    def plane_half(i):
        last = i // (chunks - 4)
        plane = (1 - last) * (i // 2) + last * (planes - 2 + i % 2)
        return plane, (1 - last) * (i % 2) + last * ((i // 2) % 2)

    def source_plane(i):
        return lax.rem(z + planes - offset(plane_half(i)[0]), planes)

    def chunk(i):
        return (source_plane(i) * 2 + plane_half(i)[1]) * span

    def whole(i):
        return pl.ds(pl.multiple_of(chunk(i), span), span)

    def piece(i, s):
        return pl.ds(pl.multiple_of(chunk(i) + s * part, part), part)

    for i in range(planes):
        there = lax.rem(z + offset(i), planes)
        block = pl.ds(pl.multiple_of(there * 2 * span, 2 * span), 2 * span)
        sendbuf[block] = nn(to_slots[block], rounded).astype(bf16)

        @pl.loop(1 if i == 0 else 0, plane_size)
        def _(k, i=i, there=there):
            target = there * plane_size + lax.rem(b_me + k, plane_size)
            copy_to(
                sendbuf.at[message(target)],
                rows_in.at[t, message(my_place)],
                zsend,
                zrecv.at[2 * i + my_half],
                {"sp": target},
            ).start()

    rows_in[t, message(my_place)] = sendbuf[message(me)]
    down_last = [
        copy_to(
            relay.at[s],
            down_w.at[pl.ds(pl.multiple_of(source * hidden_units + s * unit_half, unit_half), unit_half)],
            dsend,
            drecv.at[4 + s],
            {"tp": target},
        )
        for s, source, target in ((0, left, right), (1, right, left))
    ]
    for s in range(2):
        down_relay[s].wait_recv()
        down_last[s].start()
    gate_copy.wait()
    up_copy.wait()

    early = chunks - 4

    def ring_start(ref, i, send, recv, direct):
        for s, target, n in ((0, right, 0), (1, left, 0), (1, right, 1), (0, left, 1)):
            here = ref.at[t, piece(i, s)]
            copy_to(here, here, send, recv.at[i, n], {"tp": target}).start()

        @pl.when(i >= direct)
        def _():
            here = ref.at[t, whole(i)]
            copy_to(here, here, send, recv.at[i, 1], {"tp": opposite}).start()

    def ring_forward(ref, i, send, recv, direct):
        wait_bytes(ref.at[t, whole(i)], recv.at[i, 0])

        @pl.when(i < direct)
        def _():
            for s, source, target in ((0, left, right), (1, right, left)):
                here = ref.at[source, piece(i, s)]
                copy_to(here, here, send, recv.at[i, 1], {"tp": target}).start()

    def ring_end(ref, i, recv):
        wait_bytes(ref.at[t, pl.ds(0, 2 * span)], recv.at[i, 1])

    @pl.loop(0, chunks + 4)
    def _(i):
        @pl.when(i < chunks)
        def _():
            plane, half_of = plane_half(i)
            arrival = zrecv.at[2 * plane + half_of]
            local = (plane == 0) & (half_of == my_half)

            @pl.when(local)
            def _():
                wait_bytes(rows_in.at[t, pl.ds(0, span - 16)], arrival)

            @pl.when(jnp.logical_not(local))
            def _():
                wait_bytes(rows_in.at[t, whole(i)], arrival)

            ring_start(rows_in, i, xsend, xrecv, chunks)

        @pl.when((i >= 1) & (i < chunks + 1))
        def _():
            ring_forward(rows_in, i - 1, xsend, xrecv, chunks)

        @pl.when((i >= 2) & (i < chunks + 2))
        def _():
            j = i - 2
            ring_end(rows_in, j, xrecv)
            gate_act = jnp.zeros((span, gate_w.shape[1]), f32)
            up_act = jnp.zeros((span, gate_w.shape[1]), f32)
            squares = jnp.zeros((span, 1), f32)
            for k in range(n_tp):
                values = rows_in[k, whole(j)].astype(f32)
                squares = squares + jnp.sum(values * values, axis=1, keepdims=True)
                block = (values * ffgain_ref[k]).astype(bf16)
                gate_act = gate_act + nn(block, gate_w[k * dcols : (k + 1) * dcols])
                up_act = up_act + nn(block, up_w[k * dcols : (k + 1) * dcols])
            scale = lax.rsqrt(squares / (n_tp * dcols) + EPSILON)
            gate_act = gate_act * scale
            up_act = up_act * scale
            inner[t, whole(j)] = (silu(gate_act) * up_act).astype(bf16)
            ring_start(inner, j, isend, irecv, chunks - 1)

        @pl.when((i >= 3) & (i < chunks + 3))
        def _():
            ring_forward(inner, i - 3, isend, irecv, chunks - 1)

        @pl.when(i >= 4)
        def _():
            j = i - 4

            @pl.when(j == 0)
            def _():
                own_down.wait()
                for c in down_sends + down_last:
                    c.wait_recv()

            ring_end(inner, j, irecv)
            out = jnp.zeros((span, dcols), f32)
            for k in range(n_tp):
                out = out + nn(
                    inner[k, whole(j)], down_w[k * hidden_units : (k + 1) * hidden_units]
                )
            outs[whole(j)] = out.astype(bf16)

            @pl.loop(0, per_chunk)
            def _(k):
                y = lax.rem(b_me // 2 + k, per_chunk)
                target = source_plane(j) * plane_size + 2 * y + plane_half(j)[1]

                @pl.when(target != me)
                def _():
                    copy_to(
                        outs.at[pl.ds(pl.multiple_of(chunk(j) + y * 16, 16), 16)],
                        returned.at[message(me)],
                        rsend,
                        rrecv.at[j // early],
                        {"sp": target},
                    ).start()

    returned[message(me)] = outs[message(my_place)]
    for c in shares:
        c.wait_recv()
    eye = (
        lax.broadcasted_iota(jnp.int32, (quarter, 128), 0) == lax.broadcasted_iota(jnp.int32, (quarter, 128), 1)
    ).astype(bf16)
    shares_of = []
    for k in range(n_tp):
        p_hi, p_mid, p_lo = split3(router[k])
        shares_of.append(nt(eye, p_hi) + nt(eye, p_mid) + nt(eye, p_lo))
    share = jnp.concatenate(shares_of, axis=0)
    total = resid_ref[...]
    wait_bytes(returned.at[pl.ds(0, early * span - 16)], rrecv.at[0])
    for i in range(planes):
        if i == early // 2:
            wait_bytes(returned.at[pl.ds(0, (chunks - early) * span)], rrecv.at[1])
        there = lax.rem(z + offset(i), planes)
        block = pl.ds(pl.multiple_of(there * 2 * span, 2 * span), 2 * span)
        values = returned[block]
        for j in range(TOPK):
            total = total + share[:, j : j + 1] * nn(from_slots[j, :, block], values)
    slices[...] = total.astype(bf16)
    def columns_of(k):
        return pl.ds(pl.multiple_of(k * dcols, dcols), dcols)

    def slice_of(k):
        return slices.at[pl.ds(pl.multiple_of(k * quarter, quarter), quarter)]

    last = [
        copy_to(slice_of(other), out_ref.at[:, columns_of(t)], fsend, frecv.at[k], {"tp": other})
        for k, other in enumerate((opposite, right, left))
    ]
    for c in last:
        c.start()
    own_out = pltpu.make_async_copy(slice_of(t), out_ref.at[:, columns_of(t)], osem)
    own_out.start()
    own_out.wait()
    for c in last:
        c.wait_recv()
    wait_bytes(slices.at[pl.ds(0, 3 * quarter)], fsend)
    wait_bytes(router.at[pl.ds(0, 3)], psend)
    wait_bytes(down_w, dsend)
    wait_bytes(sendbuf.at[pl.ds(0, slots - 16)], zsend)
    wait_bytes(outs.at[pl.ds(0, slots - 16)], rsend)
    wait_bytes(rows_in.at[pl.ds(0, 3)], xsend)
    wait_bytes(inner.at[pl.ds(0, 3)], isend)
    wait_bytes(hid.at[pl.ds(0, 3)], hsend)

    @pl.when(is_owner)
    def _():
        wait_bytes(msg.at[pl.ds(0, OWNERS - 1)], msend)
        wait_bytes(carr.at[pl.ds(0, n_sp - 1)], bsend)

    @pl.when(jnp.logical_not(is_owner))
    def _():
        wait_bytes(msg.at[pl.ds(0, OWNERS)], msend)


def per_device(
    query, forget, value, gate, fmin, eld, gain, wout, stream, ffgain, routes, router,
    gate_weight, up_weight, down_weight,
):
    rows, width = query.shape
    n_sp, n_tp = lax.axis_size("sp"), lax.axis_size("tp")
    model = stream.shape[1]
    dcols = model // n_tp
    slots = n_sp * 16
    units = down_weight.shape[1]
    vmem = pl.BlockSpec(memory_space=pltpu.VMEM)
    hbm = pl.BlockSpec(memory_space=pl.ANY)
    dma = pltpu.SemaphoreType.DMA
    return pl.pallas_call(
        layer_kernel,
        name="layer",
        out_shape=jax.ShapeDtypeStruct(stream.shape, bf16),
        in_specs=[hbm] * 4 + [vmem] * 3 + [hbm, hbm] + [vmem] * 3 + [hbm] * 3,
        out_specs=hbm,
        scratch_shapes=[
            pltpu.VMEM((rows, width), bf16),
            pltpu.VMEM((rows, width), bf16),
            pltpu.VMEM((rows, width), bf16),
            pltpu.VMEM((rows, width), bf16),
            pltpu.VMEM(wout.shape, bf16),
            pltpu.VMEM((rows, dcols), bf16),
            pltpu.VMEM((OWNERS, 16, 128), bf16),
            pltpu.VMEM((n_sp, 16, 128), bf16),
            pltpu.VMEM((n_sp, 8, 128), bf16),
            pltpu.VMEM((OWNERS, 8, 128), bf16),
            pltpu.VMEM((rows, width), f32),
            pltpu.VMEM((rows, width), bf16),
            pltpu.VMEM((rows, width), bf16),
            pltpu.VMEM((n_tp, rows, width), bf16),
            pltpu.VMEM((rows, dcols), f32),
            pltpu.VMEM((model, units), bf16),
            pltpu.VMEM((model, units), bf16),
            pltpu.VMEM((n_tp * units, dcols), bf16),
            pltpu.VMEM((2, units // 2, dcols), bf16),
            pltpu.VMEM((slots, rows), bf16),
            pltpu.VMEM((TOPK, rows, slots), bf16),
            pltpu.VMEM((n_tp, 8, 128), f32),
            pltpu.VMEM((slots, dcols), bf16),
            pltpu.VMEM((n_tp, slots, dcols), bf16),
            pltpu.VMEM((n_tp, slots, units), bf16),
            pltpu.VMEM((slots, dcols), bf16),
            pltpu.VMEM((slots, dcols), bf16),
            pltpu.VMEM((rows, dcols), bf16),
            dma, dma, dma, dma, dma, dma, dma((6,)), dma((3,)), dma((3,)), dma,
            dma, dma, dma, dma, dma((6,)), dma, dma((3,)),
            dma, dma((16,)), dma, dma((16, 2)), dma, dma((16, 2)), dma, dma((2,)), dma, dma((3,)), dma((4,)), dma,
        ],
        compiler_params=pltpu.CompilerParams(
            collective_id=0, has_side_effects=True, vmem_limit_bytes=LIMIT * 2**20
        ),
    )(
        query, forget, value, gate, fmin, eld, gain, wout, stream,
        ffgain.reshape(n_tp, 1, dcols), routes.T, router.T, gate_weight, up_weight, down_weight,
    )


def solution(mesh):
    both = ("sp", "tp")
    placed = (
        P("sp", "tp"), P("sp", "tp"), P("sp", "tp"), P("sp", "tp"), P("tp"), P("tp", "sp"), P("tp"),
        P(None, "tp"), P(both, None), P(), P("sp", None), P(both, None),
        P("sp", None, "tp"), P("sp", None, "tp"), P("sp", "tp", None),
    )
    return jax.shard_map(
        per_device, mesh=mesh, in_specs=placed, out_specs=P(both, None), check_vma=False
    )
```
